512 devices in a mesh: ep: 32 (over z, x), tp: 16 (over y, core).
Axes of the slice: x: 4, y: 8, z: 8, core: 2. Of those that a mesh axis runs over, the one named last changes fastest.
Arguments:
- mixer_input: bfloat16 [16384, 2048], P('ep', 'tp'), may hold values from -6 to 6
- mixer_gain: float32 [2048], replicated, may hold values from 0.1 to 1.9
- w_query: bfloat16 [2048, 1024], P(None, 'tp'), may hold values from -0.125 to 0.125
- w_key: bfloat16 [2048, 128], replicated, may hold values from -0.125 to 0.125
- w_value: bfloat16 [2048, 128], replicated, may hold values from -0.125 to 0.125
- query_gain: float32 [64], replicated, may hold values from 0.5 to 10
- key_gain: float32 [64], replicated, may hold values from 0.5 to 10
- sink_logit: float32 [16], P('tp'), may hold values from 1 to 5
- w_output: bfloat16 [1024, 2048], P('tp'), may hold values from -0.1875 to 0.1875
- expert_input: bfloat16 [4096, 2048], P('ep'), may hold values from -6 to 6
- expert_gain: float32 [2048], replicated, may hold values from 0.1 to 1.9
- route_ids: int32 [4096, 4], P('ep'), may hold values from 0 to 31, all different within a row; in each aligned block of 128 rows (0 to 127, 128 to 255, ...) at most 32 rows name the same one
- route_weight: float32 [4096, 4], P('ep'), may hold values from 0.2 to 1.2
- expert_gate: bfloat16 [32, 2048, 2048], P('ep', None, 'tp'), may hold values from -0.125 to 0.125
- expert_up: bfloat16 [32, 2048, 2048], P('ep', None, 'tp'), may hold values from -0.125 to 0.125
- expert_down: bfloat16 [32, 2048, 2048], P('ep', None, 'tp'), may hold values from -0.125 to 0.125
- shared_gate: bfloat16 [2048, 1024], P(None, 'tp'), may hold values from -0.125 to 0.125
- shared_up: bfloat16 [2048, 1024], P(None, 'tp'), may hold values from -0.125 to 0.125
- shared_down: bfloat16 [1024, 2048], P(None, 'tp'), may hold values from -0.1875 to 0.1875
Outputs:
- mixer_output: bfloat16 [16384, 2048], P('ep', 'tp')
- expert_output: bfloat16 [4096, 2048], P('ep', 'tp')
The draws below stay inside these ranges and needn't reach their ends.
Inputs may be any that keep to these rules, and one draw needn't show every extreme that they name: `route_ids`: each row names 4 different experts. In the rows of one index of ep (aligned blocks of 128 rows) no expert is named by more than 32 rows, a bound that some block reaches.
All inputs are finite; a program needn't handle non-finite values.
Results may differ from the reference program's by a relative error of at most 0.018.
The reference program's roundings to bfloat16 on the way count: a program that leaves them out, or rounds other values in their place, can miss the bound.
Values may be sent and summed in bfloat16 or wider, within the bound.
A program may use at most 64 MiB of HBM per device.

```python
import math
import jax
import jax.numpy as jnp
import numpy as np
from jax import lax

D = 2048
HEAD = 64
Q_HEADS = 16
KV_HEADS = 2
WINDOW = 128
TOK_B = 128
TOPK = 4
FF = 2048
SHARED_FF = 1024
EXPERTS = 32
CAP = 32
TOKENS_A = 16384
TOKENS_B = 4096
N_EP = 32


def gain_draw(key):
    return jax.random.uniform(key, (HEAD,), jnp.float32, 0.6, 1.6)


def draw_query_gain(key, part):
    return gain_draw(jax.random.fold_in(key, 11))


def draw_key_gain(key, part):
    return gain_draw(jax.random.fold_in(key, 23))


def level_of(rng, extent, shards, low, largest):
    loudness = 1.0
    for position, shards_of in shards:
        steps = jax.random.uniform(jax.random.fold_in(jax.random.fold_in(rng, 6), position), (shards_of,), jnp.float32, low / len(shards), largest / len(shards))
        loudness = loudness * jnp.repeat(jnp.exp(steps), extent[position] // shards_of).reshape((-1,) + (1,) * (len(extent) - 1 - position))
    return loudness


def deal_out(stream_key, own, number, rows, count, top, most, skew):
    ranking = jax.random.permutation(stream_key, count)
    heavy_load, ordinary = portions_of(count, rows * top, most, skew, True), portions_of(count, rows * top, most, skew, False)
    places = jnp.arange(count)

    def named(sizes, rotation):
        used = int((sizes > 0).sum())
        fixed = max(1, used // 4)
        shifted = fixed + (places - fixed + rotation * (used - fixed)) % max(1, count - fixed)
        return jnp.zeros((count,), jnp.int32).at[ranking[jnp.where(places < fixed, places, shifted)]].set(jnp.asarray(sizes, jnp.int32))

    sizes = jnp.where(number % 4 == 0, named(heavy_load, number // 4), named(ordinary, number - number // 4 - 1))
    mixed = jax.random.permutation(jax.random.fold_in(own, 3), count)
    donor, taker = mixed[0:count // 2 * 2:2], mixed[1:count // 2 * 2:2]
    room = jnp.minimum(sizes[donor] - 1, most - sizes[taker]) // 2
    room = jnp.where((donor == ranking[0]) | (taker == ranking[0]) | (sizes[taker] == 0), 0, jnp.maximum(room, 0))
    shifted = jax.random.randint(jax.random.fold_in(own, 4), (count // 2,), 0, 1 << 20) % (room + 1)
    sizes = sizes.at[donor].add(-shifted).at[taker].add(shifted)
    items = jnp.searchsorted(jnp.cumsum(sizes), jnp.arange(rows * top), side="right").astype(jnp.int32)
    listing = items.reshape(top, rows).T
    listing = listing[jax.random.permutation(jax.random.fold_in(own, 1), rows)]
    rotation = jax.random.randint(jax.random.fold_in(own, 2), (rows, 1), 0, top)
    return jnp.take_along_axis(listing, (jnp.arange(top)[None, :] + rotation) % top, axis=1)


def portions_of(count, total, limit, skew, full):
    loads = [(1 << 20) // math.isqrt(grade ** skew) + 1 for grade in range(1, count + 1)]
    largest = limit if full else min(limit, max(-(-total // count), total * loads[0] // sum(loads)))
    least = 1 if total - largest >= count - 1 else 0
    holding, spare = [largest] + [least] * (count - 1), total - largest - least * (count - 1)
    while spare > 0:
        movable = [i for i in range(1, count) if holding[i] < largest] or [i for i in range(1, count) if holding[i] < limit]
        mass, remaining = sum([loads[i] for i in movable]), spare
        for i in movable:
            more = min(limit - holding[i], max(1, remaining * loads[i] // mass), spare)
            holding[i] = holding[i] + more
            spare = spare - more
    return np.array(holding)


def centred(stream_key, extent, width, bound, split=(), kind=jnp.bfloat16):
    array = jax.random.normal(stream_key, extent, jnp.float32) * width
    if len(split) > 0:
        array = level_of(stream_key, extent, split, -0.22, 0.18) * array
    return jnp.clip(array, min=-bound, max=bound).astype(kind)


def setup_inputs(seed: int = 0) -> dict:
    streams_of = jax.random.split(jax.random.key(seed), 20)
    mixer_input = centred(streams_of[0], (TOKENS_A, D), 1.0, 6.0, ((0, 32), (1, 16)))
    mixer_gain = jnp.clip(1.0 + 0.18 * jax.random.normal(streams_of[1], (D,), jnp.float32), 0.1, 1.9)
    w_query = centred(streams_of[2], (D, Q_HEADS * HEAD), D ** -0.5, 0.125, ((1, 16),))
    w_key = centred(streams_of[3], (D, KV_HEADS * HEAD), D ** -0.5, 0.125)
    w_value = centred(streams_of[4], (D, KV_HEADS * HEAD), D ** -0.5, 0.125)
    query_gain = draw_query_gain(jax.random.fold_in(streams_of[19], 71), 0)
    key_gain = draw_key_gain(jax.random.fold_in(streams_of[19], 71), 0)
    sink_logit = jnp.clip(1.0 + 4.0 * jax.random.uniform(streams_of[7], (Q_HEADS,), jnp.float32) ** level_of(streams_of[7], (Q_HEADS,), ((0, 16),), -0.2, 0.2), 1.0, 5.0)
    w_output = centred(streams_of[8], (Q_HEADS * HEAD, D), (Q_HEADS * HEAD) ** -0.5, 0.1875, ((0, 16),))
    expert_input = centred(streams_of[9], (TOKENS_B, D), 1.0, 6.0, ((0, 32),))
    expert_gain = jnp.clip(1.0 + 0.18 * jax.random.normal(streams_of[10], (D,), jnp.float32), 0.1, 1.9)
    route_ids_keys = jax.random.split(jax.random.fold_in(streams_of[11], 1), TOKENS_B // TOK_B)
    route_ids_turns = jax.random.permutation(jax.random.fold_in(streams_of[11], 3), TOKENS_B // TOK_B)
    route_ids = jax.vmap(lambda own, number: deal_out(jax.random.fold_in(streams_of[11], 2), own, number, TOK_B, EXPERTS, TOPK, CAP, 1))(route_ids_keys, route_ids_turns).reshape((TOKENS_B, TOPK))
    route_weight = jnp.clip(0.2 + 1 * jax.random.uniform(streams_of[12], (TOKENS_B, TOPK), jnp.float32) ** level_of(streams_of[12], (TOKENS_B, TOPK), ((0, 32),), -0.2, 0.2), 0.2, 1.2)
    expert_gate = centred(streams_of[13], (EXPERTS, D, FF), D ** -0.5, 0.125, ((0, 32), (2, 16)))
    expert_up = centred(streams_of[14], (EXPERTS, D, FF), D ** -0.5, 0.125, ((0, 32), (2, 16)))
    expert_down = centred(streams_of[15], (EXPERTS, FF, D), FF ** -0.5, 0.125, ((0, 32), (2, 16)))
    shared_gate = centred(streams_of[16], (D, SHARED_FF), D ** -0.5, 0.125, ((1, 16),))
    shared_up = centred(streams_of[17], (D, SHARED_FF), D ** -0.5, 0.125, ((1, 16),))
    shared_down = centred(streams_of[18], (SHARED_FF, D), SHARED_FF ** -0.5, 0.1875, ((1, 16),))
    return dict(mixer_input=mixer_input, mixer_gain=mixer_gain, w_query=w_query, w_key=w_key, w_value=w_value, query_gain=query_gain, key_gain=key_gain, sink_logit=sink_logit, w_output=w_output, expert_input=expert_input, expert_gain=expert_gain, route_ids=route_ids, route_weight=route_weight, expert_gate=expert_gate, expert_up=expert_up, expert_down=expert_down, shared_gate=shared_gate, shared_up=shared_up, shared_down=shared_down)


EPSILON = 1e-06

def head_norm(matrix, gain_vector):
    return matrix * lax.rsqrt(lax.optimization_barrier(jnp.mean(matrix * matrix, axis=-1, keepdims=True)) + EPSILON) * gain_vector

def band_attend(queries, keys_own, values_own, keys_prev, values_prev, sink_logit, first_row):
    row_count = queries.shape[0]
    head_count = queries.shape[1]
    blocks = row_count // WINDOW
    keys_all = jnp.concatenate([keys_prev, keys_own], axis=0)
    values_all = jnp.concatenate([values_prev, values_own], axis=0)
    key_band = jnp.concatenate([keys_all[:row_count].reshape(blocks, WINDOW, HEAD), keys_own.reshape(blocks, WINDOW, HEAD)], axis=1)
    value_band = jnp.concatenate([values_all[:row_count].reshape(blocks, WINDOW, HEAD), values_own.reshape(blocks, WINDOW, HEAD)], axis=1)
    query_blocks = queries.reshape(blocks, WINDOW, head_count, HEAD)
    scores = jnp.einsum('nqhd,nkd->nhqk', query_blocks.astype(jnp.float32), key_band.astype(jnp.float32)) * HEAD ** (-0.5)
    query_idx = jnp.arange(WINDOW, dtype=jnp.int32)[:, None]
    key_idx = jnp.arange(2 * WINDOW, dtype=jnp.int32)[None, :]
    relative = query_idx + WINDOW - key_idx
    block_idx = jnp.arange(blocks, dtype=jnp.int32)[:, None, None]
    key_pos = first_row + block_idx * WINDOW - WINDOW + key_idx[None]
    allowed = ((relative >= 0) & (relative < WINDOW))[None] & (key_pos >= 0)
    allowed = allowed[:, None]
    masked = jnp.where(allowed, scores, -jnp.inf)
    sink_column = sink_logit.astype(jnp.float32).reshape(1, head_count, 1, 1)
    peak_score = jnp.maximum(lax.optimization_barrier(jnp.max(masked, axis=-1, keepdims=True)), sink_column)
    exponent = jnp.exp(masked - peak_score)
    denominator = lax.optimization_barrier(jnp.sum(exponent, axis=-1, keepdims=True)) + jnp.exp(sink_column - peak_score)
    probability = (exponent / denominator).astype(jnp.bfloat16)
    mixed_rows = jnp.einsum('nhqk,nkd->nqhd', probability.astype(jnp.float32), value_band.astype(jnp.float32))
    return mixed_rows.reshape(row_count, head_count * HEAD).astype(jnp.bfloat16)

def reference(mixer_input, mixer_gain, w_query, w_key, w_value, query_gain, key_gain, sink_logit, w_output, expert_input, expert_gain, route_ids, route_weight, expert_gate, expert_up, expert_down, shared_gate, shared_up, shared_down):
    rows_float = mixer_input.astype(jnp.float32)
    scaled = (rows_float * mixer_gain).astype(jnp.bfloat16)
    inv_rms = lax.rsqrt(lax.optimization_barrier(jnp.mean(rows_float * rows_float, axis=-1, keepdims=True)) + EPSILON)
    query_raw = jnp.dot(scaled, w_query, preferred_element_type=jnp.float32)
    key_raw = jnp.dot(scaled, w_key, preferred_element_type=jnp.float32)
    value_raw = jnp.dot(scaled, w_value, preferred_element_type=jnp.float32)
    queries = head_norm(query_raw.reshape(TOKENS_A, Q_HEADS, HEAD), query_gain).astype(jnp.bfloat16)
    keys_all = head_norm(key_raw.reshape(TOKENS_A, KV_HEADS, HEAD), key_gain).astype(jnp.bfloat16)
    values_all = (value_raw * inv_rms).astype(jnp.bfloat16).reshape(TOKENS_A, KV_HEADS, HEAD)
    group_size = Q_HEADS // KV_HEADS
    zero_rows = jnp.zeros((WINDOW, HEAD), jnp.bfloat16)

    def one_head(head_index):
        kv_index = head_index // group_size
        head_query = queries[:, head_index][:, None, :]
        head_keys = keys_all[:, kv_index]
        head_values = values_all[:, kv_index]
        sink_one = sink_logit[head_index].reshape(1)
        return band_attend(head_query, head_keys, head_values, zero_rows, zero_rows, sink_one, jnp.int32(0))
    per_head = lax.map(one_head, jnp.arange(Q_HEADS, dtype=jnp.int32))
    attended = jnp.transpose(per_head, (1, 0, 2)).reshape(TOKENS_A, Q_HEADS * HEAD)
    mixer_output = jnp.dot(attended, w_output, preferred_element_type=jnp.float32).astype(jnp.bfloat16)
    expert_float = expert_input.astype(jnp.float32)
    normed = (expert_float * lax.rsqrt(lax.optimization_barrier(jnp.mean(expert_float * expert_float, axis=-1, keepdims=True)) + EPSILON) * expert_gain).astype(jnp.bfloat16)
    shared_hidden = (jax.nn.silu(jnp.dot(normed, shared_gate, preferred_element_type=jnp.float32)) * jnp.dot(normed, shared_up, preferred_element_type=jnp.float32)).astype(jnp.bfloat16)
    shared_out = jnp.dot(shared_hidden, shared_down, preferred_element_type=jnp.float32)
    ids_blocks = route_ids.reshape(N_EP, TOK_B * TOPK)
    onehot = (ids_blocks[:, :, None] == jnp.arange(EXPERTS, dtype=jnp.int32)[None, None, :]).astype(jnp.int32)
    earlier = jnp.cumsum(onehot, axis=1) - onehot
    slot_index = lax.optimization_barrier(jnp.sum(earlier * onehot, axis=-1))
    block_ids = jnp.arange(N_EP, dtype=jnp.int32)[:, None]
    slot_column = (block_ids * CAP + slot_index).astype(jnp.int32)
    token_ids = (block_ids * TOK_B + jnp.arange(TOK_B * TOPK, dtype=jnp.int32)[None] // TOPK).astype(jnp.int32)
    slot_table = jnp.full((EXPERTS, N_EP * CAP), TOKENS_B, jnp.int32).at[ids_blocks, slot_column].set(token_ids)
    padded = jnp.concatenate([normed, jnp.zeros((1, D), jnp.bfloat16)], axis=0)

    def one_expert(expert_index):
        chosen = padded[slot_table[expert_index]]
        gate_pre = jnp.dot(chosen, expert_gate[expert_index], preferred_element_type=jnp.float32)
        up_pre = jnp.dot(chosen, expert_up[expert_index], preferred_element_type=jnp.float32)
        hidden = (jax.nn.silu(gate_pre) * up_pre).astype(jnp.bfloat16)
        return jnp.dot(hidden, expert_down[expert_index], preferred_element_type=jnp.float32).astype(jnp.bfloat16)
    routed = lax.map(one_expert, jnp.arange(EXPERTS, dtype=jnp.int32))
    picked = routed[ids_blocks, slot_column].reshape(TOKENS_B, TOPK, D).astype(jnp.float32)
    expert_output = (shared_out + lax.optimization_barrier(jnp.sum(picked * route_weight[:, :, None], axis=1))).astype(jnp.bfloat16)
    return (mixer_output, expert_output)
```

```python
import functools

import jax
import jax.numpy as jnp
from jax import lax
from jax.experimental import pallas as pl
from jax.experimental.pallas import tpu as pltpu
from jax.sharding import PartitionSpec as P

HEAD = 64
WINDOW = 128
EPSILON = 1e-06
CORES = 2
X_SIZE = 4
F32 = jnp.float32
BF16 = jnp.bfloat16
MESH = pl.DeviceIdType.MESH


def mod(value, count):
    return lax.rem(value + count, count)


def dot(a, b):
    return jnp.dot(a, b, preferred_element_type=F32)


class Ring:
    def __init__(self, buf, send_sem, recv_sem, y, ny, place, pending):
        self.buf, self.send_sem, self.recv_sem = buf, send_sem, recv_sem
        self.y, self.ny, self.place, self.pending = y, ny, place, pending
        self.subs = send_sem.shape[2]
        self.half = ny // 2
        self.rows = buf.shape[1] // self.subs

    def carries(self, way, distance, sub):
        if distance < self.half:
            return True
        if distance > self.half:
            return False
        return (sub < self.subs // 2) == (way == 0)

    def copy(self, way, distance, sub):
        sign = 1 if way == 0 else -1
        part = mod(self.y - sign * (distance - 1), self.ny)
        rows = pl.ds(sub * self.rows, self.rows)
        return pltpu.make_async_remote_copy(
            src_ref=self.buf.at[part, rows],
            dst_ref=self.buf.at[part, rows],
            send_sem=self.send_sem.at[way, distance - 1, sub],
            recv_sem=self.recv_sem.at[way, distance - 1, sub],
            device_id=self.place(mod(self.y + sign, self.ny)),
            device_id_type=MESH,
        )

    def arrival(self, way, distance, sub):
        sign = 1 if way == 0 else -1
        part = mod(self.y - sign * distance, self.ny)
        rows = pl.ds(sub * self.rows, self.rows)
        return pltpu.make_async_remote_copy(
            src_ref=self.buf.at[part, rows],
            dst_ref=self.buf.at[part, rows],
            send_sem=self.send_sem.at[way, distance - 1, sub],
            recv_sem=self.recv_sem.at[way, distance - 1, sub],
            device_id=self.place(mod(self.y + sign, self.ny)),
            device_id_type=MESH,
        )

    def send(self, distance, sub, way):
        if self.carries(way, distance, sub):
            copy = self.copy(way, distance, sub)
            copy.start()
            self.pending.append(copy)

    def start(self, sub):
        for way in range(2):
            self.send(1, sub, way)

    def serve_one(self, distance, sub, way):
        if self.carries(way, distance, sub):
            self.arrival(way, distance, sub).wait_recv()
            self.send(distance + 1, sub, way)

    def serve(self, distance):
        for sub in range(self.subs):
            for way in range(2):
                self.serve_one(distance, sub, way)

    def arrived(self, distance):
        if distance < self.half:
            return [mod(self.y - distance, self.ny), mod(self.y + distance, self.ny)]
        return [mod(self.y - distance, self.ny)]


def kernel(
    n_ep,
    ny,
    nx,
    x_ref,
    gain_ref,
    wq_ref,
    wk_ref,
    wv_ref,
    qg_ref,
    kg_ref,
    sink_ref,
    wo_ref,
    ei_ref,
    eg_ref,
    ids_ref,
    rw_ref,
    gate_ref,
    up_ref,
    down_ref,
    sg_ref,
    su_ref,
    sd_ref,
    mo_ref,
    eo_ref,
    xg,
    rg,
    hg,
    ag,
    gw,
    uw,
    dw,
    wqs,
    sgs,
    sus,
    wog,
    og,
    er,
    ret,
    normed,
    gacc,
    uacc,
    oacc,
    q0acc,
    q1acc,
    kacc,
    vacc,
    ssq,
    kv,
    sk,
    mos,
    shp,
    xs_sem,
    xr_sem,
    rs_sem,
    rr_sem,
    hs_sem,
    hr_sem,
    as_sem,
    ar_sem,
    local_sem,
    pair_send,
    pair_recv,
    disp_send,
    disp_recv,
    back_send,
    back_recv,
    back_local,
    wo_send,
    wo_recv,
    halo_send,
    halo_recv,
):
    ep = lax.axis_index("ep")
    tp = lax.axis_index("tp")
    y = tp // CORES
    c = lax.rem(tp, CORES)
    other = 1 - c
    half_ny = ny // 2
    rows = x_ref.shape[0] // CORES
    toks = ei_ref.shape[0]
    dim = ei_ref.shape[1]
    cols = dim // ny
    mine = dim // (ny * CORES)
    cap = er.shape[0] // n_ep
    slots = er.shape[0]
    xi = lax.rem(ep, nx)
    pending = []

    def here(place):
        return (ep, place * CORES + c)

    partner = (ep, y * CORES + other)

    barrier = pltpu.get_barrier_semaphore()

    def greet(k, carry):
        target = lax.rem(ep + k, n_ep)
        for core in range(CORES):
            pl.semaphore_signal(
                barrier, inc=1, device_id=(target, y * CORES + core), device_id_type=MESH
            )
        return carry

    lax.fori_loop(1, n_ep, greet, 0)
    for k in range(1, ny):
        pl.semaphore_signal(barrier, inc=1, device_id=here(mod(y + k, ny)), device_id_type=MESH)
    pl.semaphore_signal(barrier, inc=1, device_id=partner, device_id_type=MESH)

    own_lanes = pl.ds(pl.multiple_of(c * mine, mine), mine)
    own_rows = pl.ds(pl.multiple_of(c * rows, rows), rows)
    other_rows = pl.ds(pl.multiple_of(other * rows, rows), rows)
    chip_lanes = pl.ds(pl.multiple_of(y * cols, cols), cols)
    wo_rows = wo_ref.shape[0]
    wo_piece = wo_rows // nx
    wo_src = pl.ds(pl.multiple_of(xi * wo_piece, wo_piece), wo_piece)
    wo_dst = pl.ds(pl.multiple_of(c * wo_rows + xi * wo_piece, wo_piece), wo_piece)
    local = [
        pltpu.make_async_copy(x_ref.at[own_rows], xg.at[y, :, own_lanes], local_sem.at[0]),
        pltpu.make_async_copy(wq_ref, wqs.at[c], local_sem.at[1]),
        pltpu.make_async_copy(sg_ref, sgs.at[c], local_sem.at[2]),
        pltpu.make_async_copy(su_ref, sus.at[c], local_sem.at[3]),
        pltpu.make_async_copy(gate_ref.at[0], gw.at[:, own_lanes], local_sem.at[4]),
        pltpu.make_async_copy(up_ref.at[0], uw.at[:, own_lanes], local_sem.at[5]),
        pltpu.make_async_copy(down_ref.at[0], dw.at[:, own_lanes], local_sem.at[6]),
        pltpu.make_async_copy(
            wo_ref.at[wo_src, chip_lanes],
            wog.at[y, wo_dst],
            local_sem.at[7],
        ),
    ]
    for copy in local:
        copy.start()
    sk[c] = jnp.full((8, 128), sink_ref[0], F32)

    expert_float = ei_ref[...].astype(F32)
    squares = jnp.mean(expert_float * expert_float, axis=-1, keepdims=True)
    normed[...] = (expert_float * lax.rsqrt(squares + EPSILON) * eg_ref[...]).astype(BF16)
    topk = ids_ref.shape[1]
    expert_idx = lax.broadcasted_iota(jnp.int32, (toks, n_ep), 1)
    named = jnp.zeros((toks, n_ep), F32)
    for k in range(topk):
        named = named + jnp.where(ids_ref[:, k : k + 1] == expert_idx, 1.0, 0.0)
    t_row = lax.broadcasted_iota(jnp.int32, (toks, toks), 0)
    t_col = lax.broadcasted_iota(jnp.int32, (toks, toks), 1)
    before = jnp.where(t_col < t_row, 1.0, 0.0).astype(BF16)
    rank = dot(before, named.astype(BF16))
    rank = jnp.where(named > 0.0, rank, -1.0)
    e_row = lax.broadcasted_iota(jnp.int32, (n_ep, slots), 0)
    e_col = lax.broadcasted_iota(jnp.int32, (n_ep, slots), 1)
    spread = jnp.where(e_col // cap == e_row, 1.0, 0.0).astype(BF16)
    slot_lane = lax.rem(lax.broadcasted_iota(jnp.int32, (toks, slots), 1), cap)

    def chosen(half):
        rank_wide = dot(rank.astype(BF16), spread).astype(jnp.int32)
        return rank_wide == slot_lane + half * cap

    pick = jnp.where(chosen(c), 1.0, 0.0).astype(BF16)
    og[...] = lax.dot_general(
        pick, normed[:, chip_lanes], (((0,), (0,)), ((), ())), preferred_element_type=F32
    ).astype(BF16)

    pl.semaphore_wait(barrier, (n_ep - 1) * CORES + (ny - 1) + 1)

    def to_partner(index, source, target):
        copy = pltpu.make_async_remote_copy(
            src_ref=source,
            dst_ref=target,
            send_sem=pair_send.at[index],
            recv_sem=pair_recv.at[index],
            device_id=partner,
            device_id_type=MESH,
        )
        return copy

    def send_partner(index, source, target):
        copy = to_partner(index, source, target)
        copy.start()
        pending.append(copy)

    other_lanes = pl.ds(pl.multiple_of(other * mine, mine), mine)
    send_partner(0, x_ref.at[other_rows], xg.at[y, :, own_lanes])
    x_in = to_partner(0, x_ref.at[other_rows], xg.at[y, :, other_lanes])

    rg_own = pltpu.make_async_copy(
        og.at[pl.ds(pl.multiple_of(ep * cap, cap), cap)],
        rg.at[y, pl.ds(0, cap)],
        disp_recv.at[0],
    )
    rg_own.start()
    r_subs = rs_sem.shape[2]
    per_sub = n_ep // r_subs

    def dispatch(k, carry):
        target = lax.rem(ep + n_ep - k, n_ep)
        pltpu.make_async_remote_copy(
            src_ref=og.at[pl.ds(pl.multiple_of(target * cap, cap), cap)],
            dst_ref=rg.at[y, pl.ds(pl.multiple_of(k * cap, cap), cap)],
            send_sem=disp_send,
            recv_sem=disp_recv.at[k // per_sub],
            device_id=(target, tp),
            device_id_type=MESH,
        ).start()
        return carry

    lax.fori_loop(1, n_ep, dispatch, 0)

    x_ring = Ring(xg, xs_sem, xr_sem, y, ny, here, pending)
    local[0].wait()
    x_in.wait_recv()
    for sub in range(x_ring.subs):
        x_ring.start(sub)

    for k in range(1, ny):
        place = mod(y + k, ny)
        copy = pltpu.make_async_remote_copy(
            src_ref=wo_ref.at[wo_src, pl.ds(pl.multiple_of(place * cols, cols), cols)],
            dst_ref=wog.at[y, wo_dst],
            send_sem=wo_send.at[k - 1],
            recv_sem=wo_recv.at[k - 1],
            device_id=here(place),
            device_id_type=MESH,
        )
        copy.start()
        pending.append(copy)

    send_partner(1, gate_ref.at[0], gw.at[:, own_lanes])
    send_partner(2, up_ref.at[0], uw.at[:, own_lanes])
    send_partner(3, wq_ref, wqs.at[c])
    send_partner(4, sg_ref, sgs.at[c])
    send_partner(5, su_ref, sus.at[c])
    send_partner(6, sk.at[c], sk.at[c])
    send_partner(7, down_ref.at[0], dw.at[:, own_lanes])
    gw_in = to_partner(1, gate_ref.at[0], gw.at[:, other_lanes])
    uw_in = to_partner(2, up_ref.at[0], uw.at[:, other_lanes])
    wq_in = to_partner(3, wq_ref, wqs.at[other])
    sg_in = to_partner(4, sg_ref, sgs.at[other])
    su_in = to_partner(5, su_ref, sus.at[other])
    sk_in = to_partner(6, sk.at[c], sk.at[other])
    dw_in = to_partner(7, down_ref.at[0], dw.at[:, other_lanes])

    for distance in range(1, half_ny + 1):
        x_ring.serve(distance)

    r_ring = Ring(rg, rs_sem, rr_sem, y, ny, here, pending)
    for sub in range(r_subs):
        landed = rg.at[y, pl.ds(sub * per_sub * cap, per_sub * cap)]
        pltpu.make_async_copy(landed, landed, disp_recv.at[sub]).wait()
        r_ring.start(sub)

    for k in range(1, ny):
        place = mod(y + k, ny)
        pltpu.make_async_remote_copy(
            src_ref=wo_ref.at[wo_src, pl.ds(pl.multiple_of(place * cols, cols), cols)],
            dst_ref=wog.at[mod(y - k, ny), wo_dst],
            send_sem=wo_send.at[k - 1],
            recv_sem=wo_recv.at[k - 1],
            device_id=here(place),
            device_id_type=MESH,
        ).wait_recv()
    local[7].wait()

    def wo_leg(k, start):
        place = ep - xi + lax.rem(xi + k, nx)
        source = wo_dst
        if not start:
            sender = lax.rem(xi + nx - k, nx)
            source = pl.ds(pl.multiple_of(c * wo_rows + sender * wo_piece, wo_piece), wo_piece)
        return pltpu.make_async_remote_copy(
            src_ref=wog.at[:, source],
            dst_ref=wog.at[:, source],
            send_sem=wo_send.at[ny - 1 + k - 1],
            recv_sem=wo_recv.at[ny - 1 + k - 1],
            device_id=(place, tp),
            device_id_type=MESH,
        )

    for k in range(1, nx):
        copy = wo_leg(k, True)
        copy.start()
        pending.append(copy)

    for copy in local[1:7]:
        copy.wait()
    wq_in.wait_recv()
    q0acc[...] = jnp.zeros_like(q0acc)
    q1acc[...] = jnp.zeros_like(q1acc)
    kacc[...] = jnp.zeros_like(kacc)
    vacc[...] = jnp.zeros_like(vacc)
    ssq[...] = jnp.zeros_like(ssq)

    def project(part, carry):
        lanes = pl.ds(pl.multiple_of(part * cols, cols), cols)
        portion = xg[part].astype(F32)
        scaled = (portion * gain_ref[:, lanes]).astype(BF16)
        ssq[...] += jnp.sum(portion * portion, axis=-1, keepdims=True)
        q0acc[...] += dot(scaled, wqs[0, lanes, :])
        q1acc[...] += dot(scaled, wqs[1, lanes, :])
        kacc[...] += dot(scaled, wk_ref[lanes, :])
        vacc[...] += dot(scaled, wv_ref[lanes, :])
        return carry

    lax.fori_loop(0, ny, project, 0)
    first_kv = y < ny // 2

    def head_of(wide):
        return jnp.where(first_kv, wide[:, :HEAD], wide[:, HEAD:])

    def head_norm(raw, gain):
        return raw * lax.rsqrt(jnp.mean(raw * raw, axis=-1, keepdims=True) + EPSILON) * gain

    inv_rms = lax.rsqrt(ssq[...] / dim + EPSILON)
    keys = head_norm(head_of(kacc[...]), kg_ref[...]).astype(BF16)
    values = (head_of(vacc[...]) * inv_rms).astype(BF16)
    kv[0, WINDOW:] = keys
    kv[1, WINDOW:] = values

    leads = jnp.logical_and(ep == 0, c == 0)
    trails = jnp.logical_and(ep == n_ep - 1, c == CORES - 1)
    after_ep = jnp.where(c == CORES - 1, lax.rem(ep + 1, n_ep), ep)
    halo = pltpu.make_async_remote_copy(
        src_ref=kv.at[:, pl.ds(rows, WINDOW)],
        dst_ref=kv.at[:, pl.ds(0, WINDOW)],
        send_sem=halo_send,
        recv_sem=halo_recv,
        device_id=(after_ep, y * CORES + other),
        device_id_type=MESH,
    )

    @pl.when(jnp.logical_not(trails))
    def _():
        halo.start()

    @pl.when(leads)
    def _():
        kv[:, :WINDOW] = jnp.zeros((2, WINDOW, HEAD), BF16)

    gw_in.wait_recv()
    uw_in.wait_recv()

    def weight_rows(part):
        return pl.ds(pl.multiple_of(part * cols, cols), cols)

    def gate_up(part, first):
        portion = rg[part]
        gate_sum = dot(portion, gw[weight_rows(part), :])
        up_sum = dot(portion, uw[weight_rows(part), :])
        if first:
            gacc[...] = gate_sum
            uacc[...] = up_sum
        else:
            gacc[...] += gate_sum
            uacc[...] += up_sum

    gate_up(y, True)

    def attend():
        @pl.when(jnp.logical_not(leads))
        def _():
            halo.wait_recv()

        sk_in.wait_recv()
        q_idx = lax.broadcasted_iota(jnp.int32, (WINDOW, 2 * WINDOW), 0)
        k_idx = lax.broadcasted_iota(jnp.int32, (WINDOW, 2 * WINDOW), 1)
        relative = q_idx + WINDOW - k_idx
        near = jnp.logical_and(relative >= 0, relative < WINDOW)
        heads = []
        for head, acc in enumerate((q0acc, q1acc)):
            queries = head_norm(acc[...], qg_ref[...]).astype(BF16)
            sink = sk[head, 0:1, 0:1]
            blocks = []
            for block in range(rows // WINDOW):
                start = block * WINDOW
                scores = lax.dot_general(
                    queries[start : start + WINDOW],
                    kv[0, start : start + 2 * WINDOW],
                    (((1,), (1,)), ((), ())),
                    preferred_element_type=F32,
                ) * HEAD ** (-0.5)
                allowed = near
                if block == 0:
                    first_key = jnp.where(leads, WINDOW, 0)
                    allowed = jnp.logical_and(near, k_idx >= first_key)
                masked = jnp.where(allowed, scores, -jnp.inf)
                peak = jnp.maximum(jnp.max(masked, axis=-1, keepdims=True), sink)
                exponent = jnp.exp(masked - peak)
                denominator = jnp.sum(exponent, axis=-1, keepdims=True) + jnp.exp(sink - peak)
                probs = (exponent / denominator).astype(BF16)
                blocks.append(dot(probs, kv[1, start : start + 2 * WINDOW]))
            heads.append(jnp.concatenate(blocks, axis=0))
        ag[y, :rows] = jnp.concatenate(heads, axis=1).astype(BF16)

    def shared_up_gate():
        sg_in.wait_recv()
        su_in.wait_recv()
        own_toks = normed[pl.ds(pl.multiple_of(c * (toks // CORES), toks // CORES), toks // CORES)]
        parts = []
        for core in range(CORES):
            gate_pre = dot(own_toks, sgs[core])
            up_pre = dot(own_toks, sus[core])
            parts.append(jax.nn.silu(gate_pre) * up_pre)
        ag[y, rows:] = jnp.concatenate(parts, axis=1).astype(BF16)

    for distance in range(1, half_ny):
        r_ring.serve(distance)
        for part in r_ring.arrived(distance):
            gate_up(part, False)
        if distance == 1:
            attend()
            for k in range(1, nx):
                wo_leg(k, False).wait_recv()
            send_partner(
                8,
                wog.at[:, pl.ds(pl.multiple_of(c * wo_rows, wo_rows), wo_rows)],
                wog.at[:, pl.ds(pl.multiple_of(c * wo_rows, wo_rows), wo_rows)],
            )
        if distance == 2:
            shared_up_gate()

    wo_other = pl.ds(pl.multiple_of(other * wo_rows, wo_rows), wo_rows)
    wo_in = to_partner(8, wog.at[:, wo_other], wog.at[:, wo_other])

    h_ring = Ring(hg, hs_sem, hr_sem, y, ny, here, pending)
    sub_rows = slots // r_subs
    far = r_ring.arrived(half_ny)[0]
    order = []
    for sub in range(r_subs // 2):
        order += [sub, sub + r_subs // 2]
    for sub in order:
        for way in range(2):
            r_ring.serve_one(half_ny, sub, way)
        at = pl.ds(sub * sub_rows, sub_rows)
        portion = rg[far, at]
        gate_pre = gacc[at] + dot(portion, gw[weight_rows(far), :])
        up_pre = uacc[at] + dot(portion, uw[weight_rows(far), :])
        hg[y, at] = (jax.nn.silu(gate_pre) * up_pre).astype(BF16)
        h_ring.start(sub)

    dw_in.wait_recv()

    def down(part, first):
        total = dot(hg[part], dw[weight_rows(part), :])
        if first:
            oacc[...] = total
        else:
            oacc[...] += total

    down(y, True)
    for distance in range(1, half_ny):
        h_ring.serve(distance)
        for part in h_ring.arrived(distance):
            down(part, False)

    a_ring = Ring(ag, as_sem, ar_sem, y, ny, here, pending)
    for sub in range(a_ring.subs):
        a_ring.start(sub)

    far = h_ring.arrived(half_ny)[0]
    back_own = pl.ds(pl.multiple_of(ep * cap, cap), cap)
    for sub in order:
        for way in range(2):
            h_ring.serve_one(half_ny, sub, way)
        at = pl.ds(sub * sub_rows, sub_rows)
        er[at] = (oacc[at] + dot(hg[far, at], dw[weight_rows(far), :])).astype(BF16)

        def back(k, carry):
            target = lax.rem(ep + k, n_ep)
            source = pl.ds(pl.multiple_of(k * cap, cap), cap)
            for core in range(CORES):
                pltpu.make_async_remote_copy(
                    src_ref=er.at[source, pl.ds(core * mine, mine)],
                    dst_ref=ret.at[c, back_own],
                    send_sem=back_send.at[core],
                    recv_sem=back_recv.at[c],
                    device_id=(target, y * CORES + core),
                    device_id_type=MESH,
                ).start()
            return carry

        lax.fori_loop(max(1, sub * per_sub), (sub + 1) * per_sub, back, 0)
        if sub == 0:
            pltpu.make_async_copy(
                er.at[pl.ds(0, cap), own_lanes], ret.at[c, back_own], back_local
            ).start()
            send_partner(9, er.at[pl.ds(0, cap), other_lanes], ret.at[c, back_own])
    back_in = to_partner(9, er.at[pl.ds(0, cap), other_lanes], ret.at[other, back_own])

    for distance in range(1, half_ny + 1):
        a_ring.serve(distance)

    shared_rows = toks // CORES
    send_partner(10, ag.at[:, pl.ds(rows, shared_rows)], shp)
    shared_in = to_partner(10, ag.at[:, pl.ds(rows, shared_rows)], shp)
    wo_in.wait_recv()
    out = jnp.zeros((rows, cols), F32)
    for part in range(ny):
        out = out + dot(ag[part, :rows], wog[part])
    out = out.astype(BF16)
    mos[0] = jnp.where(c == 0, out[:, :mine], out[:, mine:])
    mos[1] = jnp.where(c == 0, out[:, mine:], out[:, :mine])
    send_partner(11, mos.at[1], mos.at[2])
    out_in = to_partner(11, mos.at[1], mos.at[2])

    mine_sum = jnp.zeros((shared_rows, mine), F32)
    for part in range(ny):
        mine_sum = mine_sum + dot(ag[part, rows:], sd_ref[part * 2 * HEAD : (part + 1) * 2 * HEAD, :])
    shared_in.wait_recv()
    their_sum = jnp.zeros((shared_rows, mine), F32)
    for part in range(ny):
        their_sum = their_sum + dot(shp[part], sd_ref[part * 2 * HEAD : (part + 1) * 2 * HEAD, :])
    low = jnp.where(c == 0, mine_sum, their_sum)
    high = jnp.where(c == 0, their_sum, mine_sum)
    result = jnp.concatenate([low, high], axis=0)

    weight = jnp.zeros((toks, n_ep), F32)
    for k in range(topk):
        weight = weight + jnp.where(ids_ref[:, k : k + 1] == expert_idx, rw_ref[:, k : k + 1], 0.0)
    pieces = []
    for _ in range(3):
        piece = weight.astype(BF16)
        pieces.append(piece)
        weight = weight - piece.astype(F32)
    mo_ref[own_rows, :] = mos[0]

    pltpu.make_async_copy(
        er.at[pl.ds(0, cap), own_lanes], ret.at[c, back_own], back_local
    ).wait()
    back_in.wait_recv()
    elsewhere = slots - cap
    for half in range(CORES):
        landed = ret.at[half, pl.ds(0, elsewhere)]
        pltpu.make_async_copy(landed, landed, back_recv.at[half]).wait()
    for half in range(CORES):
        mask = chosen(half)
        for piece in pieces:
            spread_weight = jnp.where(mask, dot(piece, spread), 0.0).astype(BF16)
            result = result + dot(spread_weight, ret[half])
    eo_ref[...] = result.astype(BF16)

    out_in.wait_recv()
    mo_ref[other_rows, :] = mos[2]

    sent = og.at[pl.ds(0, elsewhere)]
    pltpu.make_async_copy(sent, sent, disp_send).wait()
    for core in range(CORES):
        sent = ret.at[0, pl.ds(0, elsewhere)]
        pltpu.make_async_copy(sent, sent, back_send.at[core]).wait()
    for copy in pending:
        copy.wait_send()

    @pl.when(jnp.logical_not(trails))
    def _():
        halo.wait_send()


def shards(
    mixer_input,
    mixer_gain,
    w_query,
    w_key,
    w_value,
    query_gain,
    key_gain,
    sink_logit,
    w_output,
    expert_input,
    expert_gain,
    route_ids,
    route_weight,
    expert_gate,
    expert_up,
    expert_down,
    shared_gate,
    shared_up,
    shared_down,
):
    n_ep, n_tp = lax.axis_size("ep"), lax.axis_size("tp")
    ny, nx = n_tp // CORES, min(X_SIZE, n_ep)
    rows_all, mine = mixer_input.shape
    rows = rows_all // CORES
    toks, dim = expert_input.shape
    cols = dim // ny
    slots = 2 * toks * route_ids.shape[1] // CORES
    units = expert_gate.shape[2] * CORES
    a_rows = rows + toks // CORES
    dma = pltpu.SemaphoreType.DMA
    vmem = pl.BlockSpec(memory_space=pltpu.VMEM)
    smem = pl.BlockSpec(memory_space=pltpu.SMEM)
    hbm = pl.BlockSpec(memory_space=pl.ANY)

    def ring_sems(subs):
        return [dma((2, ny // 2, subs)), dma((2, ny // 2, subs))]

    return pl.pallas_call(
        functools.partial(kernel, n_ep, ny, nx),
        name="layer",
        out_shape=(
            jax.ShapeDtypeStruct((rows_all, mine), BF16),
            jax.ShapeDtypeStruct((toks, mine), BF16),
        ),
        in_specs=[
            vmem,
            vmem,
            hbm,
            vmem,
            vmem,
            vmem,
            vmem,
            smem,
            vmem,
            vmem,
            vmem,
            vmem,
            vmem,
            hbm,
            hbm,
            hbm,
            hbm,
            hbm,
            vmem,
        ],
        out_specs=(vmem, vmem),
        scratch_shapes=[
            pltpu.VMEM((ny, rows, cols), BF16),
            pltpu.VMEM((ny, slots, cols), BF16),
            pltpu.VMEM((ny, slots, units), BF16),
            pltpu.VMEM((ny, a_rows, 2 * HEAD), BF16),
            pltpu.VMEM((dim, units), BF16),
            pltpu.VMEM((dim, units), BF16),
            pltpu.VMEM((expert_down.shape[1], cols), BF16),
            pltpu.VMEM((2,) + w_query.shape, BF16),
            pltpu.VMEM((2,) + shared_gate.shape, BF16),
            pltpu.VMEM((2,) + shared_up.shape, BF16),
            pltpu.VMEM((ny, 2 * w_output.shape[0], cols), BF16),
            pltpu.VMEM((slots, cols), BF16),
            pltpu.VMEM((slots, cols), BF16),
            pltpu.VMEM((2, slots, mine), BF16),
            pltpu.VMEM((toks, dim), BF16),
            pltpu.VMEM((slots, units), F32),
            pltpu.VMEM((slots, units), F32),
            pltpu.VMEM((slots, cols), F32),
            pltpu.VMEM((rows, HEAD), F32),
            pltpu.VMEM((rows, HEAD), F32),
            pltpu.VMEM((rows, 2 * HEAD), F32),
            pltpu.VMEM((rows, 2 * HEAD), F32),
            pltpu.VMEM((rows, 1), F32),
            pltpu.VMEM((2, WINDOW + rows, HEAD), BF16),
            pltpu.VMEM((2, 8, 128), F32),
            pltpu.VMEM((3, rows, mine), BF16),
            pltpu.VMEM((ny, toks // CORES, 2 * HEAD), BF16),
        ]
        + ring_sems(4)
        + ring_sems(4)
        + ring_sems(4)
        + ring_sems(2)
        + [
            dma((8,)),
            dma((12,)),
            dma((12,)),
            dma(()),
            dma((4,)),
            dma((2,)),
            dma((2,)),
            dma(()),
            dma((ny - 1 + nx - 1,)),
            dma((ny - 1 + nx - 1,)),
            dma(()),
            dma(()),
        ],
        compiler_params=pltpu.CompilerParams(
            collective_id=0, has_side_effects=True, vmem_limit_bytes=56 * 1024 * 1024
        ),
    )(
        mixer_input,
        mixer_gain.reshape(1, -1),
        w_query,
        w_key,
        w_value,
        query_gain.reshape(1, -1),
        key_gain.reshape(1, -1),
        sink_logit,
        w_output,
        expert_input,
        expert_gain.reshape(1, -1),
        route_ids,
        route_weight,
        expert_gate,
        expert_up,
        expert_down,
        shared_gate,
        shared_up,
        shared_down,
    )


def solution(mesh):
    in_specs = (
        P("ep", "tp"),
        P(),
        P(None, "tp"),
        P(),
        P(),
        P(),
        P(),
        P("tp"),
        P("tp", None),
        P("ep", None),
        P(),
        P("ep", None),
        P("ep", None),
        P("ep", None, "tp"),
        P("ep", None, "tp"),
        P("ep", None, "tp"),
        P(None, "tp"),
        P(None, "tp"),
        P(None, "tp"),
    )
    out_specs = (P("ep", "tp"), P("ep", "tp"))
    return jax.shard_map(shards, mesh=mesh, in_specs=in_specs, out_specs=out_specs, check_vma=False)
```

```python
import functools

import jax
import jax.numpy as jnp
from jax import lax
from jax.experimental import pallas as pl
from jax.experimental.pallas import tpu as pltpu
from jax.sharding import PartitionSpec as P

HEAD = 64
WINDOW = 128
EPSILON = 1e-06
CORES = 2
X_SIZE = 4
REACH = 2
F32 = jnp.float32
BF16 = jnp.bfloat16
MESH = pl.DeviceIdType.MESH


def mod(value, count):
    return lax.rem(value + count, count)


def dot(a, b):
    return jnp.dot(a, b, preferred_element_type=F32)


def dot_rows(a, b):
    return lax.dot_general(a, b, (((1,), (1,)), ((), ())), preferred_element_type=F32)


class Ring:
    def __init__(self, buf, send_sem, recv_sem, y, ny, place, pending, reach=None):
        self.buf, self.send_sem, self.recv_sem = buf, send_sem, recv_sem
        self.reach = reach
        self.y, self.ny, self.place, self.pending = y, ny, place, pending
        self.subs = send_sem.shape[2]
        self.half = ny // 2
        self.rows = buf.shape[1] // self.subs

    def carries(self, way, distance, sub):
        if self.reach is not None:
            return distance <= self.reach
        if distance < self.half:
            return True
        if distance > self.half:
            return False
        return (sub < self.subs // 2) == (way == 0)

    def copy(self, way, distance, sub):
        sign = 1 if way == 0 else -1
        part = mod(self.y - sign * (distance - 1), self.ny)
        rows = pl.ds(sub * self.rows, self.rows)
        return pltpu.make_async_remote_copy(
            src_ref=self.buf.at[part, rows],
            dst_ref=self.buf.at[part, rows],
            send_sem=self.send_sem.at[way, distance - 1, sub],
            recv_sem=self.recv_sem.at[way, distance - 1, sub],
            device_id=self.place(mod(self.y + sign, self.ny)),
            device_id_type=MESH,
        )

    def arrival(self, way, distance, sub):
        sign = 1 if way == 0 else -1
        part = mod(self.y - sign * distance, self.ny)
        rows = pl.ds(sub * self.rows, self.rows)
        return pltpu.make_async_remote_copy(
            src_ref=self.buf.at[part, rows],
            dst_ref=self.buf.at[part, rows],
            send_sem=self.send_sem.at[way, distance - 1, sub],
            recv_sem=self.recv_sem.at[way, distance - 1, sub],
            device_id=self.place(mod(self.y + sign, self.ny)),
            device_id_type=MESH,
        )

    def send(self, distance, sub, way):
        if self.carries(way, distance, sub):
            copy = self.copy(way, distance, sub)
            copy.start()
            self.pending.append(copy)

    def start(self, sub):
        for way in range(2):
            self.send(1, sub, way)

    def serve_one(self, distance, sub, way):
        if self.carries(way, distance, sub):
            self.arrival(way, distance, sub).wait_recv()
            self.send(distance + 1, sub, way)

    def serve(self, distance):
        for sub in range(self.subs):
            for way in range(2):
                self.serve_one(distance, sub, way)

    def arrived(self, distance):
        if distance < self.half:
            return [mod(self.y - distance, self.ny), mod(self.y + distance, self.ny)]
        return [mod(self.y - distance, self.ny)]


def kernel(
    n_ep,
    ny,
    nx,
    x_ref,
    gain_ref,
    wq_ref,
    wk_ref,
    wv_ref,
    qg_ref,
    kg_ref,
    sink_ref,
    wo_ref,
    ei_ref,
    eg_ref,
    ids_ref,
    rw_ref,
    gate_ref,
    up_ref,
    down_ref,
    sg_ref,
    su_ref,
    sd_ref,
    mo_ref,
    eo_ref,
    xg,
    xv,
    eiv,
    wkv,
    wvv,
    wov,
    sdv,
    rg,
    hg,
    ag,
    gw,
    uw,
    dw,
    wqs,
    sgs,
    sus,
    wog,
    og,
    er,
    ret,
    wide,
    macc,
    eov,
    normed,
    gacc,
    uacc,
    oacc,
    qacc,
    kacc,
    vacc,
    ssq,
    kv,
    sk,
    mos,
    shp,
    xs_sem,
    xr_sem,
    rs_sem,
    rr_sem,
    hs_sem,
    hr_sem,
    as_sem,
    ar_sem,
    local_sem,
    pair_send,
    pair_recv,
    disp_send,
    disp_recv,
    back_send,
    back_recv,
    back_local,
    wo_send,
    wo_recv,
    halo_send,
    halo_recv,
    out_sem,
):
    ep = lax.axis_index("ep")
    tp = lax.axis_index("tp")
    y = tp // CORES
    c = lax.rem(tp, CORES)
    other = 1 - c
    half_ny = ny // 2
    rows = x_ref.shape[0] // CORES
    toks = ei_ref.shape[0]
    dim = ei_ref.shape[1]
    cols = dim // ny
    mine = dim // (ny * CORES)
    cap = er.shape[0] // n_ep
    slots = er.shape[0]
    xi = lax.rem(ep, nx)
    pending = []
    far_parts = [mod(y + REACH + 1 + k, ny) for k in range(ny - 1 - 2 * REACH)]

    def here(place):
        return (ep, place * CORES + c)

    partner = (ep, y * CORES + other)

    own_lanes = pl.ds(pl.multiple_of(c * mine, mine), mine)
    other_lanes = pl.ds(pl.multiple_of(other * mine, mine), mine)
    own_head = pl.ds(pl.multiple_of(c * HEAD, HEAD), HEAD)
    other_head = pl.ds(pl.multiple_of(other * HEAD, HEAD), HEAD)
    own_rows = pl.ds(pl.multiple_of(c * rows, rows), rows)
    other_rows = pl.ds(pl.multiple_of(other * rows, rows), rows)
    wo_rows = wo_ref.shape[0]
    wo_piece = wo_rows // nx
    wo_src = pl.ds(pl.multiple_of(xi * wo_piece, wo_piece), wo_piece)
    wo_dst = pl.ds(pl.multiple_of(c * wo_rows + xi * wo_piece, wo_piece), wo_piece)
    wo_own = pl.ds(pl.multiple_of(c * wo_rows, wo_rows), wo_rows)
    wo_other = pl.ds(pl.multiple_of(other * wo_rows, wo_rows), wo_rows)

    def lanes_of(part):
        return pl.ds(pl.multiple_of(part * cols, cols), cols)

    def load(index, source, target):
        copy = pltpu.make_async_copy(source, target, local_sem.at[index])
        copy.start()
        return copy

    ei_in = load(0, ei_ref, eiv)
    xv_in = load(1, x_ref.at[other_rows], xv)
    x_own_in = load(2, x_ref.at[own_rows], xg.at[y, :, own_lanes])

    barrier = pltpu.get_barrier_semaphore()

    def greet(k, carry):
        target = lax.rem(ep + k, n_ep)
        for core in range(CORES):
            pl.semaphore_signal(
                barrier, inc=1, device_id=(target, y * CORES + core), device_id_type=MESH
            )
        return carry

    lax.fori_loop(1, n_ep, greet, 0)
    for k in range(1, ny):
        pl.semaphore_signal(barrier, inc=1, device_id=here(mod(y + k, ny)), device_id_type=MESH)
    pl.semaphore_signal(barrier, inc=1, device_id=partner, device_id_type=MESH)
    wov_in = load(3, wo_ref, wov)
    weights_in = [
        load(4, wq_ref, wqs.at[own_head]),
        load(5, wk_ref, wkv),
        load(6, wv_ref, wvv),
        load(7, gate_ref.at[0], gw.at[:, own_lanes]),
        load(8, up_ref.at[0], uw.at[:, own_lanes]),
        load(9, sg_ref, sgs.at[own_head]),
        load(10, su_ref, sus.at[own_head]),
        load(11, down_ref.at[0], dw.at[:, own_lanes]),
        load(12, sd_ref, sdv),
    ]
    sk[c] = jnp.full((8, 128), sink_ref[0], F32)

    topk = ids_ref.shape[0]
    expert_idx = lax.broadcasted_iota(jnp.int32, (n_ep, toks), 0)
    named = jnp.zeros((n_ep, toks), F32)
    for k in range(topk):
        named = named + jnp.where(ids_ref[k : k + 1, :] == expert_idx, 1.0, 0.0)
    t_row = lax.broadcasted_iota(jnp.int32, (toks, toks), 0)
    t_col = lax.broadcasted_iota(jnp.int32, (toks, toks), 1)
    before = jnp.where(t_row < t_col, 1.0, 0.0).astype(BF16)
    rank = dot(named.astype(BF16), before)
    rank = jnp.where(named > 0.0, rank, -1.0)
    e_row = lax.broadcasted_iota(jnp.int32, (slots, n_ep), 0)
    e_col = lax.broadcasted_iota(jnp.int32, (slots, n_ep), 1)
    spread = jnp.where(e_row // cap == e_col, 1.0, 0.0).astype(BF16)
    slot_row = lax.rem(lax.broadcasted_iota(jnp.int32, (slots, toks), 0), cap)
    rank_tall = dot(spread, rank.astype(BF16)).astype(jnp.int32) - slot_row
    pick = jnp.where(rank_tall == c * cap, 1.0, 0.0).astype(BF16)
    ei_in.wait()
    expert_float = eiv[...].astype(F32)
    squares = jnp.mean(expert_float * expert_float, axis=-1, keepdims=True)
    normed[...] = (expert_float * lax.rsqrt(squares + EPSILON) * eg_ref[...]).astype(BF16)
    og[0] = dot(pick, normed[:, lanes_of(y)]).astype(BF16)
    xv_in.wait()
    x_own_in.wait()

    pl.semaphore_wait(barrier, (n_ep - 1) * CORES + (ny - 1) + 1)

    def to_partner(index, source, target):
        return pltpu.make_async_remote_copy(
            src_ref=source,
            dst_ref=target,
            send_sem=pair_send.at[index],
            recv_sem=pair_recv.at[index],
            device_id=partner,
            device_id_type=MESH,
        )

    def send_partner(index, source, target):
        copy = to_partner(index, source, target)
        copy.start()
        pending.append(copy)

    send_partner(0, xv, xg.at[y, :, own_lanes])
    x_in = to_partner(0, xv, xg.at[y, :, other_lanes])

    r_subs = rs_sem.shape[2]
    per_sub = n_ep // r_subs

    def dispatch(block, part, sem_of):
        own = pltpu.make_async_copy(
            og.at[block, pl.ds(pl.multiple_of(ep * cap, cap), cap)],
            rg.at[part, pl.ds(0, cap)],
            disp_recv.at[sem_of(0)],
        )
        own.start()

        def send(k, carry):
            target = lax.rem(ep + n_ep - k, n_ep)
            pltpu.make_async_remote_copy(
                src_ref=og.at[block, pl.ds(pl.multiple_of(target * cap, cap), cap)],
                dst_ref=rg.at[part, pl.ds(pl.multiple_of(k * cap, cap), cap)],
                send_sem=disp_send.at[block],
                recv_sem=disp_recv.at[sem_of(k)],
                device_id=(target, tp),
                device_id_type=MESH,
            ).start()
            return carry

        lax.fori_loop(1, n_ep, send, 0)

    dispatch(0, y, lambda k: k // per_sub)

    x_ring = Ring(xg, xs_sem, xr_sem, y, ny, here, pending)
    x_in.wait_recv()
    for sub in range(x_ring.subs):
        x_ring.start(sub)

    for k, part in enumerate(far_parts):
        og[k + 1] = dot(pick, normed[:, lanes_of(part)]).astype(BF16)
        dispatch(k + 1, part, lambda _, k=k: r_subs + k)

    wov_in.wait()
    wo_self = pltpu.make_async_copy(
        wov.at[wo_src, lanes_of(y)], wog.at[y, wo_dst], local_sem.at[3]
    )
    wo_self.start()

    def wo_y(k, part):
        place = mod(y + k, ny)
        return pltpu.make_async_remote_copy(
            src_ref=wov.at[wo_src, lanes_of(place)],
            dst_ref=wog.at[part, wo_dst],
            send_sem=wo_send.at[k - 1],
            recv_sem=wo_recv.at[k - 1],
            device_id=here(place),
            device_id_type=MESH,
        )

    for k in range(1, ny):
        copy = wo_y(k, y)
        copy.start()
        pending.append(copy)
    for copy in weights_in:
        copy.wait()
    send_partner(3, wqs.at[own_head], wqs.at[own_head])
    send_partner(6, sk.at[c], sk.at[c])
    wq_in = to_partner(3, wqs.at[own_head], wqs.at[other_head])
    sk_in = to_partner(6, sk.at[c], sk.at[other])

    x_ring.serve(1)
    send_partner(1, gw.at[:, own_lanes], gw.at[:, own_lanes])
    send_partner(2, uw.at[:, own_lanes], uw.at[:, own_lanes])
    gw_in = to_partner(1, gw.at[:, own_lanes], gw.at[:, other_lanes])
    uw_in = to_partner(2, uw.at[:, own_lanes], uw.at[:, other_lanes])
    x_ring.serve(2)

    r_ring = Ring(rg, rs_sem, rr_sem, y, ny, here, pending, REACH)
    for sub in range(r_subs):
        landed = rg.at[y, pl.ds(sub * per_sub * cap, per_sub * cap)]
        pltpu.make_async_copy(landed, landed, disp_recv.at[sub]).wait()
        r_ring.start(sub)

    for k in range(1, ny):
        wo_y(k, mod(y - k, ny)).wait_recv()
    wo_self.wait()

    def wo_x(k, sender):
        place = ep - xi + lax.rem(xi + k, nx)
        piece = pl.ds(pl.multiple_of(c * wo_rows + sender * wo_piece, wo_piece), wo_piece)
        return pltpu.make_async_remote_copy(
            src_ref=wog.at[:, piece],
            dst_ref=wog.at[:, piece],
            send_sem=wo_send.at[ny - 1 + k - 1],
            recv_sem=wo_recv.at[ny - 1 + k - 1],
            device_id=(place, tp),
            device_id_type=MESH,
        )

    for k in range(1, nx):
        copy = wo_x(k, xi)
        copy.start()
        pending.append(copy)

    x_ring.serve(3)
    send_partner(4, sgs.at[own_head], sgs.at[own_head])
    send_partner(5, sus.at[own_head], sus.at[own_head])
    send_partner(7, dw.at[:, own_lanes], dw.at[:, own_lanes])
    sg_in = to_partner(4, sgs.at[own_head], sgs.at[other_head])
    su_in = to_partner(5, sus.at[own_head], sus.at[other_head])
    dw_in = to_partner(7, dw.at[:, own_lanes], dw.at[:, other_lanes])

    gw_in.wait_recv()
    uw_in.wait_recv()

    def weight_rows(part):
        return pl.ds(pl.multiple_of(part * cols, cols), cols)

    def gate_up(part, first):
        portion = rg[part]
        gate_sum = dot(portion, gw[weight_rows(part), :])
        up_sum = dot(portion, uw[weight_rows(part), :])
        if first:
            gacc[...] = gate_sum
            uacc[...] = up_sum
        else:
            gacc[...] += gate_sum
            uacc[...] += up_sum

    gate_up(y, True)

    for distance in range(1, REACH):
        r_ring.serve(distance)
    for distance in range(4, half_ny + 1):
        x_ring.serve(distance)

    wq_in.wait_recv()
    qacc[...] = jnp.zeros_like(qacc)
    kacc[...] = jnp.zeros_like(kacc)
    vacc[...] = jnp.zeros_like(vacc)
    ssq[...] = jnp.zeros_like(ssq)

    def project(part, carry):
        lanes = lanes_of(part)
        portion = xg[part].astype(F32)
        scaled = (portion * gain_ref[:, lanes]).astype(BF16)
        ssq[...] += jnp.sum(portion * portion, axis=-1, keepdims=True)
        qacc[...] += dot_rows(scaled, wqs[:, lanes])
        kacc[...] += dot(scaled, wkv[lanes, :])
        vacc[...] += dot(scaled, wvv[lanes, :])
        return carry

    lax.fori_loop(0, ny, project, 0)
    first_kv = y < ny // 2

    def head_of(both):
        return jnp.where(first_kv, both[:, :HEAD], both[:, HEAD:])

    def head_norm(raw, gain):
        return raw * lax.rsqrt(jnp.mean(raw * raw, axis=-1, keepdims=True) + EPSILON) * gain

    inv_rms = lax.rsqrt(ssq[...] / dim + EPSILON)
    keys = head_norm(head_of(kacc[...]), kg_ref[...]).astype(BF16)
    values = (head_of(vacc[...]) * inv_rms).astype(BF16)
    kv[0, WINDOW:] = keys
    kv[1, WINDOW:] = values

    leads = jnp.logical_and(ep == 0, c == 0)
    trails = jnp.logical_and(ep == n_ep - 1, c == CORES - 1)
    after_ep = jnp.where(c == CORES - 1, lax.rem(ep + 1, n_ep), ep)
    halo = pltpu.make_async_remote_copy(
        src_ref=kv.at[:, pl.ds(rows, WINDOW)],
        dst_ref=kv.at[:, pl.ds(0, WINDOW)],
        send_sem=halo_send,
        recv_sem=halo_recv,
        device_id=(after_ep, y * CORES + other),
        device_id_type=MESH,
    )

    @pl.when(jnp.logical_not(trails))
    def _():
        halo.start()

    @pl.when(leads)
    def _():
        kv[:, :WINDOW] = jnp.zeros((2, WINDOW, HEAD), BF16)

    for distance in range(1, REACH):
        for part in r_ring.arrived(distance):
            gate_up(part, False)

    sg_in.wait_recv()
    su_in.wait_recv()
    shared_rows = toks // CORES
    own_toks = normed[pl.ds(pl.multiple_of(c * shared_rows, shared_rows), shared_rows)]
    gate_pre = dot_rows(own_toks, sgs[...])
    up_pre = dot_rows(own_toks, sus[...])
    ag[y, rows:] = (jax.nn.silu(gate_pre) * up_pre).astype(BF16)

    @pl.when(jnp.logical_not(leads))
    def _():
        halo.wait_recv()

    sk_in.wait_recv()
    q_idx = lax.broadcasted_iota(jnp.int32, (WINDOW, 2 * WINDOW), 0)
    k_idx = lax.broadcasted_iota(jnp.int32, (WINDOW, 2 * WINDOW), 1)
    relative = q_idx + WINDOW - k_idx
    near = jnp.logical_and(relative >= 0, relative < WINDOW)
    heads = []
    for head in range(2):
        raw = qacc[:, head * HEAD : (head + 1) * HEAD]
        queries = head_norm(raw, qg_ref[...]).astype(BF16)
        sink = sk[head, 0:1, 0:1]
        blocks = []
        for block in range(rows // WINDOW):
            start = block * WINDOW
            scores = dot_rows(
                queries[start : start + WINDOW], kv[0, start : start + 2 * WINDOW]
            ) * HEAD ** (-0.5)
            allowed = near
            if block == 0:
                first_key = jnp.where(leads, WINDOW, 0)
                allowed = jnp.logical_and(near, k_idx >= first_key)
            masked = jnp.where(allowed, scores, -jnp.inf)
            peak = jnp.maximum(jnp.max(masked, axis=-1, keepdims=True), sink)
            exponent = jnp.exp(masked - peak)
            denominator = jnp.sum(exponent, axis=-1, keepdims=True) + jnp.exp(sink - peak)
            probs = (exponent / denominator).astype(BF16)
            blocks.append(dot(probs, kv[1, start : start + 2 * WINDOW]))
        heads.append(jnp.concatenate(blocks, axis=0))
    ag[y, :rows] = jnp.concatenate(heads, axis=1).astype(BF16)

    a_ring = Ring(ag, as_sem, ar_sem, y, ny, here, pending)
    for sub in range(a_ring.subs):
        a_ring.start(sub)
    for k in range(1, nx):
        wo_x(k, lax.rem(xi + nx - k, nx)).wait_recv()
    send_partner(8, wog.at[:, wo_own], wog.at[:, wo_own])
    wo_in = to_partner(8, wog.at[:, wo_other], wog.at[:, wo_other])

    for k, part in enumerate(far_parts):
        landed = rg.at[part]
        pltpu.make_async_copy(landed, landed, disp_recv.at[r_subs + k]).wait()
        gate_up(part, False)

    h_ring = Ring(hg, hs_sem, hr_sem, y, ny, here, pending)
    sub_rows = slots // r_subs
    for sub in range(r_subs):
        at = pl.ds(sub * sub_rows, sub_rows)
        gate_pre = gacc[at]
        up_pre = uacc[at]
        for way, part in enumerate(r_ring.arrived(REACH)):
            r_ring.serve_one(REACH, sub, way)
            portion = rg[part, at]
            gate_pre = gate_pre + dot(portion, gw[weight_rows(part), :])
            up_pre = up_pre + dot(portion, uw[weight_rows(part), :])
        hg[y, at] = (jax.nn.silu(gate_pre) * up_pre).astype(BF16)
        h_ring.start(sub)

    dw_in.wait_recv()

    def down(part, first):
        total = dot(hg[part], dw[weight_rows(part), :])
        if first:
            oacc[...] = total
        else:
            oacc[...] += total

    def out_part(part, first):
        total = dot(ag[part, :rows], wog[part])
        if first:
            macc[...] = total
        else:
            macc[...] += total

    down(y, True)
    wo_in.wait_recv()
    out_part(y, True)
    for distance in range(1, half_ny):
        h_ring.serve(distance)
        if distance == 1:
            a_ring.serve(1)
        for part in h_ring.arrived(distance):
            down(part, False)
        if distance == 1:
            for part in a_ring.arrived(1):
                out_part(part, False)
    a_ring.serve(2)

    order = []
    for sub in range(r_subs // 2):
        order += [sub, sub + r_subs // 2]
    last = h_ring.arrived(half_ny)[0]
    back_own = pl.ds(pl.multiple_of(ep * cap, cap), cap)
    for sub in order:
        for way in range(2):
            h_ring.serve_one(half_ny, sub, way)
        at = pl.ds(sub * sub_rows, sub_rows)
        er[at] = (oacc[at] + dot(hg[last, at], dw[weight_rows(last), :])).astype(BF16)

        def back(k, carry):
            target = lax.rem(ep + k, n_ep)
            source = pl.ds(pl.multiple_of(k * cap, cap), cap)
            for core in range(CORES):
                pltpu.make_async_remote_copy(
                    src_ref=er.at[source, pl.ds(core * mine, mine)],
                    dst_ref=ret.at[c, back_own],
                    send_sem=back_send.at[core],
                    recv_sem=back_recv.at[c],
                    device_id=(target, y * CORES + core),
                    device_id_type=MESH,
                ).start()
            return carry

        lax.fori_loop(max(1, sub * per_sub), (sub + 1) * per_sub, back, 0)
        if sub == 0:
            back_mine = pltpu.make_async_copy(
                er.at[pl.ds(0, cap), own_lanes], ret.at[c, back_own], back_local
            )
            back_mine.start()
            send_partner(9, er.at[pl.ds(0, cap), other_lanes], ret.at[c, back_own])
    back_in = to_partner(9, er.at[pl.ds(0, cap), other_lanes], ret.at[other, back_own])

    for part in a_ring.arrived(2):
        out_part(part, False)
    for distance in range(3, half_ny):
        a_ring.serve(distance)
        for part in a_ring.arrived(distance):
            out_part(part, False)

    weight = jnp.zeros((n_ep, toks), F32)
    for k in range(topk):
        weight = weight + jnp.where(ids_ref[k : k + 1, :] == expert_idx, rw_ref[k : k + 1, :], 0.0)
    n_pieces = wide.shape[0] // CORES
    for index in range(n_pieces):
        piece = weight.astype(BF16)
        weight = weight - piece.astype(F32)
        tall = dot(spread, piece)
        for half in range(CORES):
            wide[half * n_pieces + index] = jnp.transpose(
                jnp.where(rank_tall == half * cap, tall, 0.0)
            ).astype(BF16)

    a_ring.serve(half_ny)
    out_part(a_ring.arrived(half_ny)[0], False)
    send_partner(10, ag.at[:, pl.ds(rows, shared_rows)], shp)
    shared_in = to_partner(10, ag.at[:, pl.ds(rows, shared_rows)], shp)
    out = macc[...].astype(BF16)
    mos[0] = jnp.where(c == 0, out[:, :mine], out[:, mine:])
    mos[1] = jnp.where(c == 0, out[:, mine:], out[:, :mine])
    send_partner(11, mos.at[1], mos.at[2])
    out_in = to_partner(11, mos.at[1], mos.at[2])
    mo_first = pltpu.make_async_copy(mos.at[0], mo_ref.at[own_rows], out_sem.at[0])
    mo_first.start()
    mine_sum = jnp.zeros((shared_rows, mine), F32)
    for part in range(ny):
        mine_sum = mine_sum + dot(ag[part, rows:], sdv[part * 2 * HEAD : (part + 1) * 2 * HEAD, :])
    shared_in.wait_recv()
    their_sum = jnp.zeros((shared_rows, mine), F32)
    for part in range(ny):
        their_sum = their_sum + dot(shp[part], sdv[part * 2 * HEAD : (part + 1) * 2 * HEAD, :])
    low = jnp.where(c == 0, mine_sum, their_sum)
    high = jnp.where(c == 0, their_sum, mine_sum)
    result = jnp.concatenate([low, high], axis=0)

    back_mine.wait()
    back_in.wait_recv()
    elsewhere = slots - cap
    for half in range(CORES):
        landed = ret.at[half, pl.ds(0, elsewhere)]
        pltpu.make_async_copy(landed, landed, back_recv.at[half]).wait()
    for half in range(CORES):
        for index in range(n_pieces):
            result = result + dot(wide[half * n_pieces + index], ret[half])
    eov[...] = result.astype(BF16)
    eo_out = pltpu.make_async_copy(eov, eo_ref, out_sem.at[1])
    eo_out.start()
    out_in.wait_recv()
    mo_second = pltpu.make_async_copy(mos.at[2], mo_ref.at[other_rows], out_sem.at[2])
    mo_second.start()

    for block in range(len(far_parts) + 1):
        sent = og.at[block, pl.ds(0, elsewhere)]
        pltpu.make_async_copy(sent, sent, disp_send.at[block]).wait()
    for core in range(CORES):
        sent = ret.at[0, pl.ds(0, elsewhere)]
        pltpu.make_async_copy(sent, sent, back_send.at[core]).wait()
    for copy in pending:
        copy.wait_send()

    @pl.when(jnp.logical_not(trails))
    def _():
        halo.wait_send()

    mo_first.wait()
    eo_out.wait()
    mo_second.wait()


def shards(
    mixer_input,
    mixer_gain,
    w_query,
    w_key,
    w_value,
    query_gain,
    key_gain,
    sink_logit,
    w_output,
    expert_input,
    expert_gain,
    route_ids,
    route_weight,
    expert_gate,
    expert_up,
    expert_down,
    shared_gate,
    shared_up,
    shared_down,
):
    n_ep, n_tp = lax.axis_size("ep"), lax.axis_size("tp")
    ny, nx = n_tp // CORES, min(X_SIZE, n_ep)
    rows_all, mine = mixer_input.shape
    rows = rows_all // CORES
    toks, dim = expert_input.shape
    cols = dim // ny
    slots = 2 * toks * route_ids.shape[1] // CORES
    units = expert_gate.shape[2] * CORES
    a_rows = rows + toks // CORES
    dma = pltpu.SemaphoreType.DMA
    vmem = pl.BlockSpec(memory_space=pltpu.VMEM)
    smem = pl.BlockSpec(memory_space=pltpu.SMEM)
    hbm = pl.BlockSpec(memory_space=pl.ANY)

    def ring_sems(subs):
        return [dma((2, ny // 2, subs)), dma((2, ny // 2, subs))]

    return pl.pallas_call(
        functools.partial(kernel, n_ep, ny, nx),
        name="layer",
        out_shape=(
            jax.ShapeDtypeStruct((rows_all, mine), BF16),
            jax.ShapeDtypeStruct((toks, mine), BF16),
        ),
        in_specs=[
            hbm,
            vmem,
            hbm,
            hbm,
            hbm,
            vmem,
            vmem,
            smem,
            hbm,
            hbm,
            vmem,
            vmem,
            vmem,
            hbm,
            hbm,
            hbm,
            hbm,
            hbm,
            hbm,
        ],
        out_specs=(hbm, hbm),
        scratch_shapes=[
            pltpu.VMEM((ny, rows, cols), BF16),
            pltpu.VMEM((rows, mine), BF16),
            pltpu.VMEM((toks, dim), BF16),
            pltpu.VMEM(w_key.shape, BF16),
            pltpu.VMEM(w_value.shape, BF16),
            pltpu.VMEM(w_output.shape, BF16),
            pltpu.VMEM(shared_down.shape, BF16),
            pltpu.VMEM((ny, slots, cols), BF16),
            pltpu.VMEM((ny, slots, units), BF16),
            pltpu.VMEM((ny, a_rows, 2 * HEAD), BF16),
            pltpu.VMEM((dim, units), BF16),
            pltpu.VMEM((dim, units), BF16),
            pltpu.VMEM((expert_down.shape[1], cols), BF16),
            pltpu.VMEM((2 * HEAD, dim), BF16),
            pltpu.VMEM((2 * HEAD, dim), BF16),
            pltpu.VMEM((2 * HEAD, dim), BF16),
            pltpu.VMEM((ny, 2 * w_output.shape[0], cols), BF16),
            pltpu.VMEM((ny - 2 * REACH, slots, cols), BF16),
            pltpu.VMEM((slots, cols), BF16),
            pltpu.VMEM((2, slots, mine), BF16),
            pltpu.VMEM((6, toks, slots), BF16),
            pltpu.VMEM((rows, cols), F32),
            pltpu.VMEM((toks, mine), BF16),
            pltpu.VMEM((toks, dim), BF16),
            pltpu.VMEM((slots, units), F32),
            pltpu.VMEM((slots, units), F32),
            pltpu.VMEM((slots, cols), F32),
            pltpu.VMEM((rows, 2 * HEAD), F32),
            pltpu.VMEM((rows, 2 * HEAD), F32),
            pltpu.VMEM((rows, 2 * HEAD), F32),
            pltpu.VMEM((rows, 1), F32),
            pltpu.VMEM((2, WINDOW + rows, HEAD), BF16),
            pltpu.VMEM((2, 8, 128), F32),
            pltpu.VMEM((3, rows, mine), BF16),
            pltpu.VMEM((ny, toks // CORES, 2 * HEAD), BF16),
        ]
        + ring_sems(4)
        + ring_sems(4)
        + ring_sems(4)
        + ring_sems(2)
        + [
            dma((13,)),
            dma((12,)),
            dma((12,)),
            dma((ny - 2 * REACH,)),
            dma((4 + ny - 1 - 2 * REACH,)),
            dma((2,)),
            dma((2,)),
            dma(()),
            dma((ny - 1 + nx - 1,)),
            dma((ny - 1 + nx - 1,)),
            dma(()),
            dma(()),
            dma((3,)),
        ],
        compiler_params=pltpu.CompilerParams(
            collective_id=0, has_side_effects=True, vmem_limit_bytes=56 * 1024 * 1024
        ),
    )(
        mixer_input,
        mixer_gain.reshape(1, -1),
        w_query.T,
        w_key,
        w_value,
        query_gain.reshape(1, -1),
        key_gain.reshape(1, -1),
        sink_logit,
        w_output,
        expert_input,
        expert_gain.reshape(1, -1),
        route_ids.T,
        route_weight.T,
        expert_gate,
        expert_up,
        expert_down,
        shared_gate.T,
        shared_up.T,
        shared_down,
    )


def solution(mesh):
    in_specs = (
        P("ep", "tp"),
        P(),
        P(None, "tp"),
        P(),
        P(),
        P(),
        P(),
        P("tp"),
        P("tp", None),
        P("ep", None),
        P(),
        P("ep", None),
        P("ep", None),
        P("ep", None, "tp"),
        P("ep", None, "tp"),
        P("ep", None, "tp"),
        P(None, "tp"),
        P(None, "tp"),
        P(None, "tp"),
    )
    out_specs = (P("ep", "tp"), P("ep", "tp"))
    return jax.shard_map(shards, mesh=mesh, in_specs=in_specs, out_specs=out_specs, check_vma=False)
```

```python
import functools

import jax
import jax.numpy as jnp
from jax import lax
from jax.experimental import pallas as pl
from jax.experimental.pallas import tpu as pltpu
from jax.sharding import PartitionSpec as P

HEAD = 64
WINDOW = 128
EPSILON = 1e-06
CORES = 2
X_SIZE = 4
REACH = 2
SUBS = 4
ORDER = (0, 3, 1, 2)
F32 = jnp.float32
BF16 = jnp.bfloat16
MESH = pl.DeviceIdType.MESH


def mod(value, count):
    return lax.rem(value + count, count)


def dot(a, b):
    return jnp.dot(a, b, preferred_element_type=F32)


def dot_rows(a, b):
    return lax.dot_general(a, b, (((1,), (1,)), ((), ())), preferred_element_type=F32)


class Ring:
    def __init__(self, buf, send_sem, recv_sem, y, ny, place, subs, reach=None):
        self.buf, self.send_sem, self.recv_sem = buf, send_sem, recv_sem
        self.y, self.ny, self.place = y, ny, place
        self.subs, self.reach = subs, reach
        self.half = ny // 2
        self.rows = buf.shape[1] // subs

    def carries(self, way, distance, sub):
        if self.reach is not None:
            return distance <= self.reach
        if distance < self.half:
            return True
        if distance > self.half:
            return False
        return (sub < self.subs // 2) == (way == 0)

    def copy(self, way, distance, sub, origin):
        sign = 1 if way == 0 else -1
        part = mod(self.y - sign * origin, self.ny)
        rows = pl.ds(sub * self.rows, self.rows)
        index = (distance - 1) * self.subs * 2 + sub * 2 + way
        if self.reach is None and distance == self.half:
            index = (distance - 1) * self.subs * 2 + sub
        return pltpu.make_async_remote_copy(
            src_ref=self.buf.at[part, rows],
            dst_ref=self.buf.at[part, rows],
            send_sem=self.send_sem,
            recv_sem=self.recv_sem.at[index],
            device_id=self.place(mod(self.y + sign, self.ny)),
            device_id_type=MESH,
        )

    def send(self, distance, sub, way):
        if self.carries(way, distance, sub):
            self.copy(way, distance, sub, distance - 1).start()

    def start(self, sub):
        for way in range(2):
            self.send(1, sub, way)

    def serve_one(self, distance, sub, way):
        if self.carries(way, distance, sub):
            self.copy(way, distance, sub, distance).wait_recv()
            self.send(distance + 1, sub, way)

    def serve(self, distance, order=None):
        for sub in order or range(self.subs):
            for way in range(2):
                self.serve_one(distance, sub, way)

    def arrived(self, distance):
        if distance < self.half:
            return [mod(self.y - distance, self.ny), mod(self.y + distance, self.ny)]
        return [mod(self.y - distance, self.ny)]

    def finish(self):
        count = self.ny - 1 if self.reach is None else 2 * self.reach
        sent = self.buf.at[pl.ds(0, count)]
        pltpu.make_async_copy(sent, sent, self.send_sem).wait()


def kernel(
    n_ep,
    ny,
    nx,
    x_ref,
    gain_in,
    wq_ref,
    wk_ref,
    wv_ref,
    qg_in,
    kg_in,
    sink_in,
    wo_ref,
    ei_ref,
    eg_in,
    ids_in,
    rw_in,
    gate_ref,
    up_ref,
    down_ref,
    sg_ref,
    su_ref,
    sd_ref,
    mo_ref,
    eo_ref,
    xg,
    gain_ref,
    qg_ref,
    kg_ref,
    sink_ref,
    eg_ref,
    ids_ref,
    rw_ref,
    xv,
    eiv,
    wkv,
    wvv,
    wov,
    sdv,
    rg,
    hg,
    ag,
    gw,
    uw,
    dw,
    wqs,
    sgs,
    sus,
    wog,
    og,
    er,
    ret,
    wide,
    macc,
    eov,
    normed,
    oacc,
    qacc,
    kacc,
    vacc,
    ssq,
    kv,
    sk,
    mos,
    shp,
    xs_sem,
    xr_sem,
    rs_sem,
    rr_sem,
    hs_sem,
    hr_sem,
    as_sem,
    ar_sem,
    local_sem,
    pair_send,
    pair_recv,
    disp_send,
    disp_recv,
    back_send,
    back_recv,
    back_local,
    wo_send,
    wo_recv,
    halo_send,
    halo_recv,
    out_sem,
):
    ep = lax.axis_index("ep")
    tp = lax.axis_index("tp")
    y = tp // CORES
    c = lax.rem(tp, CORES)
    other = 1 - c
    half_ny = ny // 2
    rows = x_ref.shape[0] // CORES
    toks = ei_ref.shape[0]
    dim = ei_ref.shape[1]
    cols = dim // ny
    mine = dim // (ny * CORES)
    cap = er.shape[0] // n_ep
    slots = er.shape[0]
    xi = lax.rem(ep, nx)
    pending = []
    far_parts = [mod(y + REACH + 1 + k, ny) for k in range(ny - 1 - 2 * REACH)]

    def here(place):
        return (ep, place * CORES + c)

    partner = (ep, y * CORES + other)

    own_lanes = pl.ds(pl.multiple_of(c * mine, mine), mine)
    other_lanes = pl.ds(pl.multiple_of(other * mine, mine), mine)
    own_head = pl.ds(pl.multiple_of(c * HEAD, HEAD), HEAD)
    other_head = pl.ds(pl.multiple_of(other * HEAD, HEAD), HEAD)
    own_rows = pl.ds(pl.multiple_of(c * rows, rows), rows)
    other_rows = pl.ds(pl.multiple_of(other * rows, rows), rows)
    wo_rows = wo_ref.shape[0]
    wo_piece = wo_rows // nx
    wo_src = pl.ds(pl.multiple_of(xi * wo_piece, wo_piece), wo_piece)
    wo_dst = pl.ds(pl.multiple_of(c * wo_rows + xi * wo_piece, wo_piece), wo_piece)
    wo_own = pl.ds(pl.multiple_of(c * wo_rows, wo_rows), wo_rows)
    wo_other = pl.ds(pl.multiple_of(other * wo_rows, wo_rows), wo_rows)

    def lanes_of(part):
        return pl.ds(pl.multiple_of(part * cols, cols), cols)

    def load(index, source, target):
        copy = pltpu.make_async_copy(source, target, local_sem.at[index])
        copy.start()
        return copy

    ids_load = load(13, ids_in, ids_ref)
    ei_in = load(0, ei_ref, eiv)
    eg_load = load(14, eg_in, eg_ref)
    xv_in = load(1, x_ref.at[other_rows], xv)
    x_own_in = load(2, x_ref.at[own_rows], xg.at[y, :, own_lanes])
    wov_in = load(3, wo_ref, wov)
    sink_load = load(19, sink_in, sink_ref)

    barrier = pltpu.get_barrier_semaphore()

    def greet(k, carry):
        target = lax.rem(ep + k, n_ep)
        for core in range(CORES):
            pl.semaphore_signal(
                barrier, inc=1, device_id=(target, y * CORES + core), device_id_type=MESH
            )
        return carry

    lax.fori_loop(1, n_ep, greet, 0)
    for k in range(1, ny):
        pl.semaphore_signal(barrier, inc=1, device_id=here(mod(y + k, ny)), device_id_type=MESH)
    pl.semaphore_signal(barrier, inc=1, device_id=partner, device_id_type=MESH)
    small = [
        load(15, rw_in, rw_ref),
        load(16, gain_in, gain_ref),
        load(17, qg_in, qg_ref),
        load(18, kg_in, kg_ref),
    ]
    weights_in = [
        load(4, wq_ref, wqs.at[own_head]),
        load(5, wk_ref, wkv),
        load(6, wv_ref, wvv),
        load(7, gate_ref.at[0], gw.at[:, own_lanes]),
        load(8, up_ref.at[0], uw.at[:, own_lanes]),
        load(9, sg_ref, sgs.at[own_head]),
        load(10, su_ref, sus.at[own_head]),
        load(11, down_ref.at[0], dw.at[:, own_lanes]),
        load(12, sd_ref, sdv),
    ]
    sink_load.wait()
    sk[c] = jnp.full((8, 128), sink_ref[0], F32)

    ids_load.wait()
    topk = ids_ref.shape[0]
    expert_idx = lax.broadcasted_iota(jnp.int32, (n_ep, toks), 0)
    named = jnp.zeros((n_ep, toks), F32)
    for k in range(topk):
        named = named + jnp.where(ids_ref[k : k + 1, :] == expert_idx, 1.0, 0.0)
    t_row = lax.broadcasted_iota(jnp.int32, (toks, toks), 0)
    t_col = lax.broadcasted_iota(jnp.int32, (toks, toks), 1)
    before = jnp.where(t_row < t_col, 1.0, 0.0).astype(BF16)
    rank = dot(named.astype(BF16), before)
    rank = jnp.where(named > 0.0, rank, -1.0)
    e_row = lax.broadcasted_iota(jnp.int32, (slots, n_ep), 0)
    e_col = lax.broadcasted_iota(jnp.int32, (slots, n_ep), 1)
    spread = jnp.where(e_row // cap == e_col, 1.0, 0.0).astype(BF16)
    slot_row = lax.rem(lax.broadcasted_iota(jnp.int32, (slots, toks), 0), cap)
    rank_tall = dot(spread, rank.astype(BF16)).astype(jnp.int32) - slot_row
    pick = jnp.where(rank_tall == c * cap, 1.0, 0.0).astype(BF16)
    ei_in.wait()
    eg_load.wait()
    expert_float = eiv[...].astype(F32)
    squares = jnp.mean(expert_float * expert_float, axis=-1, keepdims=True)
    normed[...] = (expert_float * lax.rsqrt(squares + EPSILON) * eg_ref[...]).astype(BF16)
    og[0] = dot(pick, normed[:, lanes_of(y)]).astype(BF16)
    xv_in.wait()
    x_own_in.wait()

    pl.semaphore_wait(barrier, (n_ep - 1) * CORES + (ny - 1) + 1)

    def to_partner(index, source, target):
        return pltpu.make_async_remote_copy(
            src_ref=source,
            dst_ref=target,
            send_sem=pair_send.at[index],
            recv_sem=pair_recv.at[index],
            device_id=partner,
            device_id_type=MESH,
        )

    def send_partner(index, source, target):
        copy = to_partner(index, source, target)
        copy.start()
        pending.append(copy)

    send_partner(0, xv, xg.at[y, :, own_lanes])
    x_in = to_partner(0, xv, xg.at[y, :, other_lanes])

    wov_in.wait()
    wo_self = pltpu.make_async_copy(
        wov.at[wo_src, lanes_of(y)], wog.at[y, wo_dst], local_sem.at[3]
    )
    wo_self.start()

    def wo_y(k, part):
        place = mod(y + k, ny)
        return pltpu.make_async_remote_copy(
            src_ref=wov.at[wo_src, lanes_of(place)],
            dst_ref=wog.at[part, wo_dst],
            send_sem=wo_send.at[0],
            recv_sem=wo_recv.at[0],
            device_id=here(place),
            device_id_type=MESH,
        )

    for k in range(1, ny):
        wo_y(k, y).start()
    r_subs = SUBS
    sub_rows = slots // r_subs
    per_sub = n_ep // r_subs

    def dispatch(blocks, parts, base):
        for block, part in zip(blocks, parts):
            pltpu.make_async_copy(
                og.at[block, pl.ds(pl.multiple_of(ep * cap, cap), cap)],
                rg.at[part, pl.ds(0, cap)],
                disp_recv.at[base],
            ).start()

        for sub in ORDER:

            def send(k, carry, sub=sub):
                target = lax.rem(ep + n_ep - k, n_ep)
                for block, part in zip(blocks, parts):
                    pltpu.make_async_remote_copy(
                        src_ref=og.at[block, pl.ds(pl.multiple_of(target * cap, cap), cap)],
                        dst_ref=rg.at[part, pl.ds(pl.multiple_of(k * cap, cap), cap)],
                        send_sem=disp_send.at[block],
                        recv_sem=disp_recv.at[base + sub],
                        device_id=(target, tp),
                        device_id_type=MESH,
                    ).start()
                return carry

            lax.fori_loop(max(1, sub * per_sub), (sub + 1) * per_sub, send, 0)

    dispatch([0], [y], 0)

    x_ring = Ring(xg, xs_sem, xr_sem, y, ny, here, 4)
    x_in.wait_recv()
    for sub in range(x_ring.subs):
        x_ring.start(sub)

    for k, part in enumerate(far_parts):
        og[k + 1] = dot(pick, normed[:, lanes_of(part)]).astype(BF16)

    for copy in weights_in + small:
        copy.wait()
    send_partner(3, wqs.at[own_head], wqs.at[own_head])
    send_partner(6, sk.at[c], sk.at[c])
    wq_in = to_partner(3, wqs.at[own_head], wqs.at[other_head])
    sk_in = to_partner(6, sk.at[c], sk.at[other])

    x_ring.serve(1)

    dispatch(range(1, len(far_parts) + 1), far_parts, r_subs)
    send_partner(1, gw.at[:, own_lanes], gw.at[:, own_lanes])
    send_partner(2, uw.at[:, own_lanes], uw.at[:, own_lanes])
    gw_in = to_partner(1, gw.at[:, own_lanes], gw.at[:, other_lanes])
    uw_in = to_partner(2, uw.at[:, own_lanes], uw.at[:, other_lanes])

    r_ring = Ring(rg, rs_sem, rr_sem, y, ny, here, r_subs, REACH)

    def r_start(sub):
        landed = rg.at[y, pl.ds(sub * per_sub * cap, per_sub * cap)]
        pltpu.make_async_copy(landed, landed, disp_recv.at[sub]).wait()
        r_ring.start(sub)

    r_start(ORDER[0])

    x_ring.serve(2)

    for sub in ORDER[1:]:
        r_start(sub)

    wo_y_bytes = og.at[0, pl.ds(0, (ny - 1) * wo_piece)]
    pltpu.make_async_copy(wo_y_bytes, wo_y_bytes, wo_recv.at[0]).wait()
    wo_self.wait()

    def wo_x(k, sender):
        place = ep - xi + lax.rem(xi + k, nx)
        piece = pl.ds(pl.multiple_of(c * wo_rows + sender * wo_piece, wo_piece), wo_piece)
        return pltpu.make_async_remote_copy(
            src_ref=wog.at[:, piece],
            dst_ref=wog.at[:, piece],
            send_sem=wo_send.at[1],
            recv_sem=wo_recv.at[1],
            device_id=(place, tp),
            device_id_type=MESH,
        )

    wo_x_bytes = wog.at[:, pl.ds(0, (nx - 1) * wo_piece)]
    for k in range(1, nx):
        wo_x(k, xi).start()

    x_ring.serve(3)
    send_partner(4, sgs.at[own_head], sgs.at[own_head])
    send_partner(5, sus.at[own_head], sus.at[own_head])
    send_partner(7, dw.at[:, own_lanes], dw.at[:, own_lanes])
    sg_in = to_partner(4, sgs.at[own_head], sgs.at[other_head])
    su_in = to_partner(5, sus.at[own_head], sus.at[other_head])
    dw_in = to_partner(7, dw.at[:, own_lanes], dw.at[:, other_lanes])

    for distance in range(1, REACH):
        r_ring.serve(distance, ORDER)
    def weight_rows(part):
        return pl.ds(pl.multiple_of(part * cols, cols), cols)

    h_ring = Ring(hg, hs_sem, hr_sem, y, ny, here, r_subs)
    near_parts = [y]
    for distance in range(1, REACH + 1):
        near_parts += r_ring.arrived(distance)

    def hidden(sub):
        for way in range(2):
            r_ring.serve_one(REACH, sub, way)
        landed = rg.at[pl.ds(0, len(far_parts)), pl.ds(0, sub_rows)]
        pltpu.make_async_copy(landed, landed, disp_recv.at[r_subs + sub]).wait()
        at = pl.ds(sub * sub_rows, sub_rows)
        gate_pre = jnp.zeros((sub_rows, gw.shape[1]), F32)
        up_pre = jnp.zeros((sub_rows, uw.shape[1]), F32)
        for part in near_parts + far_parts:
            portion = rg[part, at]
            gate_pre = gate_pre + dot(portion, gw[weight_rows(part), :])
            up_pre = up_pre + dot(portion, uw[weight_rows(part), :])
        hg[y, at] = (jax.nn.silu(gate_pre) * up_pre).astype(BF16)
        h_ring.start(sub)

    gw_in.wait_recv()
    uw_in.wait_recv()
    hidden(ORDER[0])

    for distance in range(4, half_ny + 1):
        x_ring.serve(distance)

    wq_in.wait_recv()
    qacc[...] = jnp.zeros_like(qacc)
    kacc[...] = jnp.zeros_like(kacc)
    vacc[...] = jnp.zeros_like(vacc)
    ssq[...] = jnp.zeros_like(ssq)

    def project(part, carry):
        lanes = lanes_of(part)
        portion = xg[part].astype(F32)
        scaled = (portion * gain_ref[:, lanes]).astype(BF16)
        ssq[...] += jnp.sum(portion * portion, axis=-1, keepdims=True)
        qacc[...] += dot_rows(scaled, wqs[:, lanes])
        kacc[...] += dot(scaled, wkv[lanes, :])
        vacc[...] += dot(scaled, wvv[lanes, :])
        return carry

    lax.fori_loop(0, ny // 2, project, 0)

    hidden(ORDER[1])

    lax.fori_loop(ny // 2, ny, project, 0)
    first_kv = y < ny // 2

    def head_of(both):
        return jnp.where(first_kv, both[:, :HEAD], both[:, HEAD:])

    def head_norm(raw, gain):
        return raw * lax.rsqrt(jnp.mean(raw * raw, axis=-1, keepdims=True) + EPSILON) * gain

    inv_rms = lax.rsqrt(ssq[...] / dim + EPSILON)
    keys = head_norm(head_of(kacc[...]), kg_ref[...]).astype(BF16)
    values = (head_of(vacc[...]) * inv_rms).astype(BF16)
    kv[0, WINDOW:] = keys
    kv[1, WINDOW:] = values

    leads = jnp.logical_and(ep == 0, c == 0)
    trails = jnp.logical_and(ep == n_ep - 1, c == CORES - 1)
    after_ep = jnp.where(c == CORES - 1, lax.rem(ep + 1, n_ep), ep)
    halo = pltpu.make_async_remote_copy(
        src_ref=kv.at[:, pl.ds(rows, WINDOW)],
        dst_ref=kv.at[:, pl.ds(0, WINDOW)],
        send_sem=halo_send,
        recv_sem=halo_recv,
        device_id=(after_ep, y * CORES + other),
        device_id_type=MESH,
    )

    @pl.when(jnp.logical_not(trails))
    def _():
        halo.start()

    @pl.when(leads)
    def _():
        kv[:, :WINDOW] = jnp.zeros((2, WINDOW, HEAD), BF16)

    hidden(ORDER[2])
    h_ring.serve(1, ORDER[:2])

    sg_in.wait_recv()
    su_in.wait_recv()
    shared_rows = toks // CORES
    own_toks = normed[pl.ds(pl.multiple_of(c * shared_rows, shared_rows), shared_rows)]
    gate_pre = dot_rows(own_toks, sgs[...])
    up_pre = dot_rows(own_toks, sus[...])
    ag[y, rows:] = (jax.nn.silu(gate_pre) * up_pre).astype(BF16)

    q_idx = lax.broadcasted_iota(jnp.int32, (WINDOW, 2 * WINDOW), 0)
    k_idx = lax.broadcasted_iota(jnp.int32, (WINDOW, 2 * WINDOW), 1)
    relative = q_idx + WINDOW - k_idx
    near = jnp.logical_and(relative >= 0, relative < WINDOW)
    first_key = jnp.where(leads, WINDOW, 0)

    @pl.when(jnp.logical_not(leads))
    def _():
        halo.wait_recv()

    sk_in.wait_recv()

    def attend(block):
        start = block * WINDOW
        allowed = near
        if block == 0:
            allowed = jnp.logical_and(near, k_idx >= first_key)
        heads = []
        for head in range(2):
            raw = qacc[start : start + WINDOW, head * HEAD : (head + 1) * HEAD]
            queries = head_norm(raw, qg_ref[...]).astype(BF16)
            sink = sk[head, 0:1, 0:1]
            scores = dot_rows(queries, kv[0, start : start + 2 * WINDOW]) * HEAD ** (-0.5)
            masked = jnp.where(allowed, scores, -jnp.inf)
            peak = jnp.maximum(jnp.max(masked, axis=-1, keepdims=True), sink)
            exponent = jnp.exp(masked - peak)
            denominator = jnp.sum(exponent, axis=-1, keepdims=True) + jnp.exp(sink - peak)
            probs = (exponent / denominator).astype(BF16)
            heads.append(dot(probs, kv[1, start : start + 2 * WINDOW]))
        ag[y, start : start + WINDOW] = jnp.concatenate(heads, axis=1).astype(BF16)

    for block in range(rows // WINDOW):
        attend(block)
    hidden(ORDER[3])

    h_ring.serve(1, ORDER[2:3])
    h_ring.serve(2, ORDER[:2])
    h_ring.serve(1, ORDER[3:])
    h_ring.serve(2, ORDER[2:])

    a_ring = Ring(ag, as_sem, ar_sem, y, ny, here, 2)
    for sub in range(a_ring.subs):
        a_ring.start(sub)

    pltpu.make_async_copy(wo_x_bytes, wo_x_bytes, wo_recv.at[1]).wait()
    send_partner(8, wog.at[:, wo_own], wog.at[:, wo_own])
    wo_in = to_partner(8, wog.at[:, wo_other], wog.at[:, wo_other])
    dw_in.wait_recv()

    def out_part(part, first):
        total = dot(ag[part, :rows], wog[part])
        if first:
            macc[...] = total
        else:
            macc[...] += total

    seven = [y]
    for distance in range(1, half_ny):
        seven += h_ring.arrived(distance)
    for distance in range(3, half_ny):
        for sub in ORDER:
            h_ring.serve(distance, (sub,))
            at = pl.ds(sub * sub_rows, sub_rows)
            total = jnp.zeros((sub_rows, cols), F32)
            for part in seven:
                total = total + dot(hg[part, at], dw[weight_rows(part), :])
            oacc[at] = total
    a_ring.serve(1)
    wo_in.wait_recv()
    out_part(y, True)

    last = h_ring.arrived(half_ny)[0]
    back_own = pl.ds(pl.multiple_of(ep * cap, cap), cap)
    for sub in ORDER:
        for way in range(2):
            h_ring.serve_one(half_ny, sub, way)
        at = pl.ds(sub * sub_rows, sub_rows)
        er[at] = (oacc[at] + dot(hg[last, at], dw[weight_rows(last), :])).astype(BF16)

        def back(k, carry):
            target = lax.rem(ep + k, n_ep)
            source = pl.ds(pl.multiple_of(k * cap, cap), cap)
            for core in range(CORES):
                pltpu.make_async_remote_copy(
                    src_ref=er.at[source, pl.ds(core * mine, mine)],
                    dst_ref=ret.at[c, back_own],
                    send_sem=back_send.at[core],
                    recv_sem=back_recv.at[c],
                    device_id=(target, y * CORES + core),
                    device_id_type=MESH,
                ).start()
            return carry

        lax.fori_loop(max(1, sub * per_sub), (sub + 1) * per_sub, back, 0)
        if sub == 0:
            back_mine = pltpu.make_async_copy(
                er.at[pl.ds(0, cap), own_lanes], ret.at[c, back_own], back_local
            )
            back_mine.start()
            send_partner(9, er.at[pl.ds(0, cap), other_lanes], ret.at[c, back_own])
    back_in = to_partner(9, er.at[pl.ds(0, cap), other_lanes], ret.at[other, back_own])

    for part in a_ring.arrived(1):
        out_part(part, False)
    for distance in range(2, half_ny):
        a_ring.serve(distance)
        for part in a_ring.arrived(distance):
            out_part(part, False)

    weight = jnp.zeros((n_ep, toks), F32)
    for k in range(topk):
        weight = weight + jnp.where(ids_ref[k : k + 1, :] == expert_idx, rw_ref[k : k + 1, :], 0.0)
    n_pieces = wide.shape[0] // CORES
    for index in range(n_pieces):
        piece = weight.astype(BF16)
        weight = weight - piece.astype(F32)
        tall = dot(spread, piece)
        for half in range(CORES):
            wide[half * n_pieces + index] = jnp.transpose(
                jnp.where(rank_tall == half * cap, tall, 0.0)
            ).astype(BF16)

    a_ring.serve(half_ny)
    out_part(a_ring.arrived(half_ny)[0], False)
    send_partner(10, ag.at[:, pl.ds(rows, shared_rows)], shp)
    shared_in = to_partner(10, ag.at[:, pl.ds(rows, shared_rows)], shp)
    out = macc[...].astype(BF16)
    mos[0] = jnp.where(c == 0, out[:, :mine], out[:, mine:])
    mos[1] = jnp.where(c == 0, out[:, mine:], out[:, :mine])
    send_partner(11, mos.at[1], mos.at[2])
    out_in = to_partner(11, mos.at[1], mos.at[2])
    mo_first = pltpu.make_async_copy(mos.at[0], mo_ref.at[own_rows], out_sem.at[0])
    mo_first.start()
    mine_sum = jnp.zeros((shared_rows, mine), F32)
    for part in range(ny):
        mine_sum = mine_sum + dot(ag[part, rows:], sdv[part * 2 * HEAD : (part + 1) * 2 * HEAD, :])
    shared_in.wait_recv()
    their_sum = jnp.zeros((shared_rows, mine), F32)
    for part in range(ny):
        their_sum = their_sum + dot(shp[part], sdv[part * 2 * HEAD : (part + 1) * 2 * HEAD, :])
    low = jnp.where(c == 0, mine_sum, their_sum)
    high = jnp.where(c == 0, their_sum, mine_sum)
    result = jnp.concatenate([low, high], axis=0)

    back_mine.wait()
    back_in.wait_recv()
    elsewhere = slots - cap
    for half in range(CORES):
        landed = ret.at[half, pl.ds(0, elsewhere)]
        pltpu.make_async_copy(landed, landed, back_recv.at[half]).wait()
    for half in range(CORES):
        for index in range(n_pieces):
            result = result + dot(wide[half * n_pieces + index], ret[half])
    eov[...] = result.astype(BF16)
    eo_out = pltpu.make_async_copy(eov, eo_ref, out_sem.at[1])
    eo_out.start()
    out_in.wait_recv()
    mo_second = pltpu.make_async_copy(mos.at[2], mo_ref.at[other_rows], out_sem.at[2])
    mo_second.start()

    for block in range(len(far_parts) + 1):
        sent = og.at[block, pl.ds(0, elsewhere)]
        pltpu.make_async_copy(sent, sent, disp_send.at[block]).wait()
    for core in range(CORES):
        sent = ret.at[0, pl.ds(0, elsewhere)]
        pltpu.make_async_copy(sent, sent, back_send.at[core]).wait()
    for ring in (x_ring, r_ring, h_ring, a_ring):
        ring.finish()
    pltpu.make_async_copy(wo_y_bytes, wo_y_bytes, wo_send.at[0]).wait()
    pltpu.make_async_copy(wo_x_bytes, wo_x_bytes, wo_send.at[1]).wait()
    for copy in pending:
        copy.wait_send()

    @pl.when(jnp.logical_not(trails))
    def _():
        halo.wait_send()

    mo_first.wait()
    eo_out.wait()
    mo_second.wait()


def shards(
    mixer_input,
    mixer_gain,
    w_query,
    w_key,
    w_value,
    query_gain,
    key_gain,
    sink_logit,
    w_output,
    expert_input,
    expert_gain,
    route_ids,
    route_weight,
    expert_gate,
    expert_up,
    expert_down,
    shared_gate,
    shared_up,
    shared_down,
):
    n_ep, n_tp = lax.axis_size("ep"), lax.axis_size("tp")
    ny, nx = n_tp // CORES, min(X_SIZE, n_ep)
    rows_all, mine = mixer_input.shape
    rows = rows_all // CORES
    toks, dim = expert_input.shape
    cols = dim // ny
    slots = 2 * toks * route_ids.shape[1] // CORES
    units = expert_gate.shape[2] * CORES
    a_rows = rows + toks // CORES
    dma = pltpu.SemaphoreType.DMA
    hbm = pl.BlockSpec(memory_space=pltpu.HBM)
    anywhere = pl.BlockSpec(memory_space=pl.ANY)

    def ring_sems(subs, parts):
        return [dma(()), dma((subs * parts,))]

    return pl.pallas_call(
        functools.partial(kernel, n_ep, ny, nx),
        name="layer",
        out_shape=(
            jax.ShapeDtypeStruct((rows_all, mine), BF16),
            jax.ShapeDtypeStruct((toks, mine), BF16),
        ),
        in_specs=[hbm] * 19,
        out_specs=(anywhere, anywhere),
        scratch_shapes=[
            pltpu.VMEM((ny, rows, cols), BF16),
            pltpu.VMEM((1, dim), F32),
            pltpu.VMEM((1, HEAD), F32),
            pltpu.VMEM((1, HEAD), F32),
            pltpu.SMEM((1,), F32),
            pltpu.VMEM((1, dim), F32),
            pltpu.VMEM(route_ids.shape[::-1], jnp.int32),
            pltpu.VMEM(route_ids.shape[::-1], F32),
            pltpu.VMEM((rows, mine), BF16),
            pltpu.VMEM((toks, dim), BF16),
            pltpu.VMEM(w_key.shape, BF16),
            pltpu.VMEM(w_value.shape, BF16),
            pltpu.VMEM(w_output.shape, BF16),
            pltpu.VMEM(shared_down.shape, BF16),
            pltpu.VMEM((ny, slots, cols), BF16),
            pltpu.VMEM((ny, slots, units), BF16),
            pltpu.VMEM((ny, a_rows, 2 * HEAD), BF16),
            pltpu.VMEM((dim, units), BF16),
            pltpu.VMEM((dim, units), BF16),
            pltpu.VMEM((expert_down.shape[1], cols), BF16),
            pltpu.VMEM((2 * HEAD, dim), BF16),
            pltpu.VMEM((2 * HEAD, dim), BF16),
            pltpu.VMEM((2 * HEAD, dim), BF16),
            pltpu.VMEM((ny, 2 * w_output.shape[0], cols), BF16),
            pltpu.VMEM((ny - 2 * REACH, slots, cols), BF16),
            pltpu.VMEM((slots, cols), BF16),
            pltpu.VMEM((2, slots, mine), BF16),
            pltpu.VMEM((6, toks, slots), BF16),
            pltpu.VMEM((rows, cols), F32),
            pltpu.VMEM((toks, mine), BF16),
            pltpu.VMEM((toks, dim), BF16),
            pltpu.VMEM((slots, cols), F32),
            pltpu.VMEM((rows, 2 * HEAD), F32),
            pltpu.VMEM((rows, 2 * HEAD), F32),
            pltpu.VMEM((rows, 2 * HEAD), F32),
            pltpu.VMEM((rows, 1), F32),
            pltpu.VMEM((2, WINDOW + rows, HEAD), BF16),
            pltpu.VMEM((2, 8, 128), F32),
            pltpu.VMEM((3, rows, mine), BF16),
            pltpu.VMEM((ny, toks // CORES, 2 * HEAD), BF16),
        ]
        + ring_sems(SUBS, ny - 1)
        + ring_sems(SUBS, 2 * REACH)
        + ring_sems(SUBS, ny - 1)
        + ring_sems(2, ny - 1)
        + [
            dma((20,)),
            dma((12,)),
            dma((12,)),
            dma((ny - 2 * REACH,)),
            dma((2 * SUBS,)),
            dma((2,)),
            dma((2,)),
            dma(()),
            dma((2,)),
            dma((2,)),
            dma(()),
            dma(()),
            dma((3,)),
        ],
        compiler_params=pltpu.CompilerParams(
            collective_id=0, has_side_effects=True, vmem_limit_bytes=56 * 1024 * 1024
        ),
    )(
        mixer_input,
        mixer_gain.reshape(1, -1),
        w_query.T,
        w_key,
        w_value,
        query_gain.reshape(1, -1),
        key_gain.reshape(1, -1),
        sink_logit,
        w_output,
        expert_input,
        expert_gain.reshape(1, -1),
        route_ids.T,
        route_weight.T,
        expert_gate,
        expert_up,
        expert_down,
        shared_gate.T,
        shared_up.T,
        shared_down,
    )


def solution(mesh):
    in_specs = (
        P("ep", "tp"),
        P(),
        P(None, "tp"),
        P(),
        P(),
        P(),
        P(),
        P("tp"),
        P("tp", None),
        P("ep", None),
        P(),
        P("ep", None),
        P("ep", None),
        P("ep", None, "tp"),
        P("ep", None, "tp"),
        P("ep", None, "tp"),
        P(None, "tp"),
        P(None, "tp"),
        P(None, "tp"),
    )
    out_specs = (P("ep", "tp"), P("ep", "tp"))
    return jax.shard_map(shards, mesh=mesh, in_specs=in_specs, out_specs=out_specs, check_vma=False)
```

```python
import functools

import jax
import jax.numpy as jnp
from jax import lax
from jax.experimental import pallas as pl
from jax.experimental.pallas import tpu as pltpu
from jax.sharding import PartitionSpec as P

HEAD = 64
WINDOW = 128
EPSILON = 1e-06
CORES = 2
X_SIZE = 4
REACH = 2
SUBS = 4
ORDER = (0, 3, 1, 2)
FURTHER = ()
F32 = jnp.float32
BF16 = jnp.bfloat16
MESH = pl.DeviceIdType.MESH


def mod(value, count):
    return lax.rem(value + count, count)


def dot(a, b):
    return jnp.dot(a, b, preferred_element_type=F32)


def dot_rows(a, b):
    return lax.dot_general(a, b, (((1,), (1,)), ((), ())), preferred_element_type=F32)


class Ring:
    def __init__(self, buf, send_sem, recv_sem, y, ny, place, subs, reach=None, further=()):
        self.further = further
        self.buf, self.send_sem, self.recv_sem = buf, send_sem, recv_sem
        self.y, self.ny, self.place = y, ny, place
        self.subs, self.reach = subs, reach
        self.half = ny // 2
        self.rows = buf.shape[1] // subs

    def carries(self, way, distance, sub):
        if self.reach is not None:
            return distance <= self.reach + (sub in self.further)
        if distance < self.half:
            return True
        if distance > self.half:
            return False
        return (sub < self.subs // 2) == (way == 0)

    def copy(self, way, distance, sub, origin):
        sign = 1 if way == 0 else -1
        part = mod(self.y - sign * origin, self.ny)
        rows = pl.ds(sub * self.rows, self.rows)
        index = (distance - 1) * self.subs * 2 + sub * 2 + way
        if self.reach is None and distance == self.half:
            index = (distance - 1) * self.subs * 2 + sub
        return pltpu.make_async_remote_copy(
            src_ref=self.buf.at[part, rows],
            dst_ref=self.buf.at[part, rows],
            send_sem=self.send_sem,
            recv_sem=self.recv_sem.at[index],
            device_id=self.place(mod(self.y + sign, self.ny)),
            device_id_type=MESH,
        )

    def send(self, distance, sub, way):
        if self.carries(way, distance, sub):
            self.copy(way, distance, sub, distance - 1).start()

    def start(self, sub):
        for way in range(2):
            self.send(1, sub, way)

    def serve_one(self, distance, sub, way):
        if self.carries(way, distance, sub):
            self.copy(way, distance, sub, distance).wait_recv()
            self.send(distance + 1, sub, way)

    def serve(self, distance, order=None):
        for sub in order or range(self.subs):
            for way in range(2):
                self.serve_one(distance, sub, way)

    def arrived(self, distance):
        if distance < self.half:
            return [mod(self.y - distance, self.ny), mod(self.y + distance, self.ny)]
        return [mod(self.y - distance, self.ny)]

    def finish(self):
        pieces = (self.ny - 1) * self.subs
        if self.reach is not None:
            pieces = 2 * (self.reach * self.subs + len(self.further))
        high = max(k for k in range(1, self.subs + 1) if pieces % k == 0)
        sent = self.buf.at[pl.ds(0, pieces // high), pl.ds(0, high * self.rows)]
        pltpu.make_async_copy(sent, sent, self.send_sem).wait()


def kernel(
    n_ep,
    ny,
    nx,
    x_ref,
    gain_in,
    wq_ref,
    wk_ref,
    wv_ref,
    qg_in,
    kg_in,
    sink_in,
    wo_ref,
    ei_ref,
    eg_in,
    ids_in,
    rw_in,
    gate_ref,
    up_ref,
    down_ref,
    sg_ref,
    su_ref,
    sd_ref,
    mo_ref,
    eo_ref,
    xg,
    gain_ref,
    qg_ref,
    kg_ref,
    sink_ref,
    eg_ref,
    ids_ref,
    rw_ref,
    xv,
    eiv,
    wkv,
    wvv,
    wov,
    sdv,
    rg,
    hg,
    ag,
    gw,
    uw,
    dw,
    wqs,
    sgs,
    sus,
    wog,
    og,
    er,
    ret,
    wide,
    macc,
    eov,
    normed,
    oacc,
    qacc,
    kacc,
    vacc,
    ssq,
    kv,
    sk,
    mos,
    shp,
    xs_sem,
    xr_sem,
    rs_sem,
    rr_sem,
    hs_sem,
    hr_sem,
    as_sem,
    ar_sem,
    local_sem,
    pair_send,
    pair_recv,
    disp_send,
    disp_recv,
    back_send,
    back_recv,
    back_local,
    wo_send,
    wo_recv,
    halo_send,
    halo_recv,
    out_sem,
):
    ep = lax.axis_index("ep")
    tp = lax.axis_index("tp")
    y = tp // CORES
    c = lax.rem(tp, CORES)
    other = 1 - c
    half_ny = ny // 2
    rows = x_ref.shape[0] // CORES
    toks = ei_ref.shape[0]
    dim = ei_ref.shape[1]
    cols = dim // ny
    mine = dim // (ny * CORES)
    cap = er.shape[0] // n_ep
    slots = er.shape[0]
    xi = lax.rem(ep, nx)
    pending = []
    far_parts = [mod(y + REACH + 1 + k, ny) for k in range(ny - 1 - 2 * REACH)]

    def here(place):
        return (ep, place * CORES + c)

    partner = (ep, y * CORES + other)

    own_lanes = pl.ds(pl.multiple_of(c * mine, mine), mine)
    other_lanes = pl.ds(pl.multiple_of(other * mine, mine), mine)
    own_head = pl.ds(pl.multiple_of(c * HEAD, HEAD), HEAD)
    other_head = pl.ds(pl.multiple_of(other * HEAD, HEAD), HEAD)
    own_rows = pl.ds(pl.multiple_of(c * rows, rows), rows)
    other_rows = pl.ds(pl.multiple_of(other * rows, rows), rows)
    wo_rows = wo_ref.shape[0]
    wo_piece = wo_rows // nx
    wo_src = pl.ds(pl.multiple_of(xi * wo_piece, wo_piece), wo_piece)
    wo_dst = pl.ds(pl.multiple_of(c * wo_rows + xi * wo_piece, wo_piece), wo_piece)
    wo_own = pl.ds(pl.multiple_of(c * wo_rows, wo_rows), wo_rows)
    wo_other = pl.ds(pl.multiple_of(other * wo_rows, wo_rows), wo_rows)

    def lanes_of(part):
        return pl.ds(pl.multiple_of(part * cols, cols), cols)

    def load(index, source, target):
        copy = pltpu.make_async_copy(source, target, local_sem.at[index])
        copy.start()
        return copy

    ids_load = load(13, ids_in, ids_ref)
    ei_in = load(0, ei_ref, eiv)
    eg_load = load(14, eg_in, eg_ref)
    xv_in = load(1, x_ref.at[other_rows], xv)
    x_own_in = load(2, x_ref.at[own_rows], xg.at[y, :, own_lanes])
    wov_in = load(3, wo_ref, wov)
    sink_load = load(19, sink_in, sink_ref)

    barrier = pltpu.get_barrier_semaphore()

    def greet(k, carry):
        target = lax.rem(ep + k, n_ep)
        for core in range(CORES):
            pl.semaphore_signal(
                barrier, inc=1, device_id=(target, y * CORES + core), device_id_type=MESH
            )
        return carry

    lax.fori_loop(n_ep // 4, n_ep, greet, 0)
    lax.fori_loop(1, n_ep // 4, greet, 0)
    for k in range(1, ny):
        pl.semaphore_signal(barrier, inc=1, device_id=here(mod(y + k, ny)), device_id_type=MESH)
    pl.semaphore_signal(barrier, inc=1, device_id=partner, device_id_type=MESH)
    small = [
        load(15, rw_in, rw_ref),
        load(16, gain_in, gain_ref),
        load(17, qg_in, qg_ref),
        load(18, kg_in, kg_ref),
    ]
    weights_in = [
        load(4, wq_ref, wqs.at[own_head]),
        load(5, wk_ref, wkv),
        load(6, wv_ref, wvv),
        load(7, gate_ref.at[0], gw.at[:, own_lanes]),
        load(8, up_ref.at[0], uw.at[:, own_lanes]),
        load(9, sg_ref, sgs.at[own_head]),
        load(10, su_ref, sus.at[own_head]),
        load(11, down_ref.at[0], dw.at[:, own_lanes]),
        load(12, sd_ref, sdv),
    ]
    sink_load.wait()
    sk[c] = jnp.full((8, 128), sink_ref[0], F32)

    ids_load.wait()
    topk = ids_ref.shape[0]
    expert_idx = lax.broadcasted_iota(jnp.int32, (n_ep, toks), 0)
    named = jnp.zeros((n_ep, toks), F32)
    for k in range(topk):
        named = named + jnp.where(ids_ref[k : k + 1, :] == expert_idx, 1.0, 0.0)
    t_row = lax.broadcasted_iota(jnp.int32, (toks, toks), 0)
    t_col = lax.broadcasted_iota(jnp.int32, (toks, toks), 1)
    before = jnp.where(t_row < t_col, 1.0, 0.0).astype(BF16)
    rank = dot(named.astype(BF16), before)
    rank = jnp.where(named > 0.0, rank, -1.0)
    e_row = lax.broadcasted_iota(jnp.int32, (slots, n_ep), 0)
    e_col = lax.broadcasted_iota(jnp.int32, (slots, n_ep), 1)
    spread = jnp.where(e_row // cap == e_col, 1.0, 0.0).astype(BF16)
    slot_row = lax.rem(lax.broadcasted_iota(jnp.int32, (slots, toks), 0), cap)
    rank_tall = dot(spread, rank.astype(BF16)).astype(jnp.int32) - slot_row
    pick = jnp.where(rank_tall == c * cap, 1.0, 0.0).astype(BF16)
    ei_in.wait()
    eg_load.wait()
    expert_float = eiv[...].astype(F32)
    squares = jnp.mean(expert_float * expert_float, axis=-1, keepdims=True)
    normed[...] = (expert_float * lax.rsqrt(squares + EPSILON) * eg_ref[...]).astype(BF16)
    og[0] = dot(pick, normed[:, lanes_of(y)]).astype(BF16)
    xv_in.wait()
    x_own_in.wait()

    pl.semaphore_wait(barrier, (n_ep - 1) * CORES + (ny - 1) + 1)

    def to_partner(index, source, target):
        return pltpu.make_async_remote_copy(
            src_ref=source,
            dst_ref=target,
            send_sem=pair_send.at[index],
            recv_sem=pair_recv.at[index],
            device_id=partner,
            device_id_type=MESH,
        )

    def send_partner(index, source, target):
        copy = to_partner(index, source, target)
        copy.start()
        pending.append(copy)

    send_partner(0, xv, xg.at[y, :, own_lanes])
    x_in = to_partner(0, xv, xg.at[y, :, other_lanes])

    zi = ep // nx
    nz = n_ep // nx
    away = zi > 0
    wov_in.wait()
    wo_place = mod(y + zi, ny)
    wo_self = pltpu.make_async_copy(
        wov.at[wo_src, lanes_of(wo_place)], wog.at[y, wo_dst], local_sem.at[3]
    )
    wo_y = pltpu.make_async_remote_copy(
        src_ref=wov.at[wo_src, lanes_of(wo_place)],
        dst_ref=wog.at[y, wo_dst],
        send_sem=wo_send.at[0],
        recv_sem=wo_recv.at[0],
        device_id=here(wo_place),
        device_id_type=MESH,
    )

    @pl.when(away)
    def _():
        wo_y.start()

    @pl.when(jnp.logical_not(away))
    def _():
        wo_self.start()

    r_subs = SUBS
    sub_rows = slots // r_subs
    per_sub = n_ep // r_subs

    def direct(far, sub):
        return sub not in FURTHER or 0 < far < len(far_parts) - 1

    def dispatch(blocks, parts, base):
        for block, part in zip(blocks, parts):
            pltpu.make_async_copy(
                og.at[block, pl.ds(pl.multiple_of(ep * cap, cap), cap)],
                rg.at[part, pl.ds(0, cap)],
                disp_recv.at[base],
            ).start()

        for sub in ORDER:

            def send(k, carry, sub=sub):
                target = lax.rem(ep + n_ep - k, n_ep)
                for block, part in zip(blocks, parts):
                    if base and not direct(block - 1, sub):
                        continue
                    pltpu.make_async_remote_copy(
                        src_ref=og.at[block, pl.ds(pl.multiple_of(target * cap, cap), cap)],
                        dst_ref=rg.at[part, pl.ds(pl.multiple_of(k * cap, cap), cap)],
                        send_sem=disp_send.at[block],
                        recv_sem=disp_recv.at[base + sub],
                        device_id=(target, tp),
                        device_id_type=MESH,
                    ).start()
                return carry

            lax.fori_loop(max(1, sub * per_sub), (sub + 1) * per_sub, send, 0)

    dispatch([0], [y], 0)

    x_ring = Ring(xg, xs_sem, xr_sem, y, ny, here, 4)
    x_in.wait_recv()
    for sub in range(x_ring.subs):
        x_ring.start(sub)

    for k, part in enumerate(far_parts):
        og[k + 1] = dot(pick, normed[:, lanes_of(part)]).astype(BF16)
    dispatch(range(1, len(far_parts) + 1), far_parts, r_subs)

    for copy in weights_in + small:
        copy.wait()
    send_partner(3, wqs.at[own_head], wqs.at[own_head])
    send_partner(6, sk.at[c], sk.at[c])
    wq_in = to_partner(3, wqs.at[own_head], wqs.at[other_head])
    sk_in = to_partner(6, sk.at[c], sk.at[other])

    x_ring.serve(1)

    send_partner(1, gw.at[:, own_lanes], gw.at[:, own_lanes])
    send_partner(2, uw.at[:, own_lanes], uw.at[:, own_lanes])
    gw_in = to_partner(1, gw.at[:, own_lanes], gw.at[:, other_lanes])
    uw_in = to_partner(2, uw.at[:, own_lanes], uw.at[:, other_lanes])

    r_ring = Ring(rg, rs_sem, rr_sem, y, ny, here, r_subs, REACH, FURTHER)

    def r_start(sub):
        landed = rg.at[y, pl.ds(sub * per_sub * cap, per_sub * cap)]
        pltpu.make_async_copy(landed, landed, disp_recv.at[sub]).wait()
        r_ring.start(sub)

    r_start(ORDER[0])

    x_ring.serve(2)

    for sub in ORDER[1:]:
        r_start(sub)

    x_ring.serve(3)
    send_partner(4, sgs.at[own_head], sgs.at[own_head])
    send_partner(5, sus.at[own_head], sus.at[own_head])
    send_partner(7, dw.at[:, own_lanes], dw.at[:, own_lanes])
    sg_in = to_partner(4, sgs.at[own_head], sgs.at[other_head])
    su_in = to_partner(5, sus.at[own_head], sus.at[other_head])
    dw_in = to_partner(7, dw.at[:, own_lanes], dw.at[:, other_lanes])

    for distance in range(1, REACH):
        r_ring.serve(distance, ORDER)
    def weight_rows(part):
        return pl.ds(pl.multiple_of(part * cols, cols), cols)

    h_ring = Ring(hg, hs_sem, hr_sem, y, ny, here, r_subs)
    near_parts = [y]
    for distance in range(1, REACH + 1):
        near_parts += r_ring.arrived(distance)

    def hidden(sub):
        for way in range(2):
            if sub in FURTHER:
                r_ring.serve_one(REACH + 1, sub, way)
            else:
                r_ring.serve_one(REACH, sub, way)
        n_direct = sum(direct(far, sub) for far in range(len(far_parts)))
        landed = rg.at[pl.ds(0, n_direct), pl.ds(0, sub_rows)]
        pltpu.make_async_copy(landed, landed, disp_recv.at[r_subs + sub]).wait()
        at = pl.ds(sub * sub_rows, sub_rows)
        gate_pre = jnp.zeros((sub_rows, gw.shape[1]), F32)
        up_pre = jnp.zeros((sub_rows, uw.shape[1]), F32)
        for part in near_parts + far_parts:
            portion = rg[part, at]
            gate_pre = gate_pre + dot(portion, gw[weight_rows(part), :])
            up_pre = up_pre + dot(portion, uw[weight_rows(part), :])
        hg[y, at] = (jax.nn.silu(gate_pre) * up_pre).astype(BF16)
        h_ring.start(sub)

    gw_in.wait_recv()
    uw_in.wait_recv()
    hidden(ORDER[0])

    for distance in range(4, half_ny + 1):
        x_ring.serve(distance)

    wq_in.wait_recv()
    qacc[...] = jnp.zeros_like(qacc)
    kacc[...] = jnp.zeros_like(kacc)
    vacc[...] = jnp.zeros_like(vacc)
    ssq[...] = jnp.zeros_like(ssq)

    def project(part, carry):
        lanes = lanes_of(part)
        portion = xg[part].astype(F32)
        scaled = (portion * gain_ref[:, lanes]).astype(BF16)
        ssq[...] += jnp.sum(portion * portion, axis=-1, keepdims=True)
        qacc[...] += dot_rows(scaled, wqs[:, lanes])
        kacc[...] += dot(scaled, wkv[lanes, :])
        vacc[...] += dot(scaled, wvv[lanes, :])
        return carry

    lax.fori_loop(0, ny // 2, project, 0)

    hidden(ORDER[1])

    lax.fori_loop(ny // 2, ny, project, 0)
    first_kv = y < ny // 2

    def head_of(both):
        return jnp.where(first_kv, both[:, :HEAD], both[:, HEAD:])

    def head_norm(raw, gain):
        return raw * lax.rsqrt(jnp.mean(raw * raw, axis=-1, keepdims=True) + EPSILON) * gain

    inv_rms = lax.rsqrt(ssq[...] / dim + EPSILON)
    keys = head_norm(head_of(kacc[...]), kg_ref[...]).astype(BF16)
    values = (head_of(vacc[...]) * inv_rms).astype(BF16)
    kv[0, WINDOW:] = keys
    kv[1, WINDOW:] = values

    leads = jnp.logical_and(ep == 0, c == 0)
    trails = jnp.logical_and(ep == n_ep - 1, c == CORES - 1)
    after_ep = jnp.where(c == CORES - 1, lax.rem(ep + 1, n_ep), ep)
    halo = pltpu.make_async_remote_copy(
        src_ref=kv.at[:, pl.ds(rows, WINDOW)],
        dst_ref=kv.at[:, pl.ds(0, WINDOW)],
        send_sem=halo_send,
        recv_sem=halo_recv,
        device_id=(after_ep, y * CORES + other),
        device_id_type=MESH,
    )

    @pl.when(jnp.logical_not(trails))
    def _():
        halo.start()

    @pl.when(leads)
    def _():
        kv[:, :WINDOW] = jnp.zeros((2, WINDOW, HEAD), BF16)

    for sub in FURTHER:
        for way in range(2):
            r_ring.serve_one(REACH, sub, way)

    hidden(ORDER[2])
    h_ring.serve(1, ORDER[:2])

    sg_in.wait_recv()
    su_in.wait_recv()
    shared_rows = toks // CORES
    own_toks = normed[pl.ds(pl.multiple_of(c * shared_rows, shared_rows), shared_rows)]
    gate_pre = dot_rows(own_toks, sgs[...])
    up_pre = dot_rows(own_toks, sus[...])
    ag[y, rows:] = (jax.nn.silu(gate_pre) * up_pre).astype(BF16)

    q_idx = lax.broadcasted_iota(jnp.int32, (WINDOW, 2 * WINDOW), 0)
    k_idx = lax.broadcasted_iota(jnp.int32, (WINDOW, 2 * WINDOW), 1)
    relative = q_idx + WINDOW - k_idx
    near = jnp.logical_and(relative >= 0, relative < WINDOW)
    first_key = jnp.where(leads, WINDOW, 0)

    @pl.when(jnp.logical_not(leads))
    def _():
        halo.wait_recv()

    sk_in.wait_recv()

    def attend(block):
        start = block * WINDOW
        allowed = near
        if block == 0:
            allowed = jnp.logical_and(near, k_idx >= first_key)
        heads = []
        for head in range(2):
            raw = qacc[start : start + WINDOW, head * HEAD : (head + 1) * HEAD]
            queries = head_norm(raw, qg_ref[...]).astype(BF16)
            sink = sk[head, 0:1, 0:1]
            scores = dot_rows(queries, kv[0, start : start + 2 * WINDOW]) * HEAD ** (-0.5)
            masked = jnp.where(allowed, scores, -jnp.inf)
            peak = jnp.maximum(jnp.max(masked, axis=-1, keepdims=True), sink)
            exponent = jnp.exp(masked - peak)
            denominator = jnp.sum(exponent, axis=-1, keepdims=True) + jnp.exp(sink - peak)
            probs = (exponent / denominator).astype(BF16)
            heads.append(dot(probs, kv[1, start : start + 2 * WINDOW]))
        ag[y, start : start + WINDOW] = jnp.concatenate(heads, axis=1).astype(BF16)

    wo_part = mod(y - zi, ny)

    @pl.when(away)
    def _():
        wo_y.wait()

    @pl.when(jnp.logical_not(away))
    def _():
        wo_self.wait()

    wo_z_bytes = og.at[0, pl.ds(0, (nz - 1) * wo_piece)]
    for k in range(1, nz):
        pltpu.make_async_remote_copy(
            src_ref=wog.at[wo_part, wo_dst],
            dst_ref=wog.at[wo_part, wo_dst],
            send_sem=wo_send.at[1],
            recv_sem=wo_recv.at[1],
            device_id=(lax.rem(ep + k * nx, n_ep), tp),
            device_id_type=MESH,
        ).start()

    for block in range(rows // WINDOW):
        attend(block)

    a_ring = Ring(ag, as_sem, ar_sem, y, ny, here, 2)
    for sub in range(a_ring.subs):
        a_ring.start(sub)

    hidden(ORDER[3])

    h_ring.serve(1, ORDER[2:3])
    h_ring.serve(2, ORDER[:2])
    h_ring.serve(1, ORDER[3:])
    h_ring.serve(2, ORDER[2:])

    pltpu.make_async_copy(wo_z_bytes, wo_z_bytes, wo_recv.at[1]).wait()
    wo_x_bytes = wog.at[:, pl.ds(0, (nx - 1) * wo_piece)]
    for k in range(1, nx):
        pltpu.make_async_remote_copy(
            src_ref=wog.at[:, wo_dst],
            dst_ref=wog.at[:, wo_dst],
            send_sem=wo_send.at[2],
            recv_sem=wo_recv.at[2],
            device_id=(ep - xi + lax.rem(xi + k, nx), tp),
            device_id_type=MESH,
        ).start()

    def out_part(part, first):
        total = dot(ag[part, :rows], wog[part])
        if first:
            macc[...] = total
        else:
            macc[...] += total

    a_ring.serve(1)
    dw_in.wait_recv()

    seven = [y]
    for distance in range(1, half_ny):
        seven += h_ring.arrived(distance)
    for distance in range(3, half_ny):
        for sub in ORDER:
            h_ring.serve(distance, (sub,))
            at = pl.ds(sub * sub_rows, sub_rows)
            total = jnp.zeros((sub_rows, cols), F32)
            for part in seven:
                total = total + dot(hg[part, at], dw[weight_rows(part), :])
            oacc[at] = total
    a_ring.serve(2)

    pltpu.make_async_copy(wo_x_bytes, wo_x_bytes, wo_recv.at[2]).wait()
    send_partner(8, wog.at[:, wo_own], wog.at[:, wo_own])
    wo_in = to_partner(8, wog.at[:, wo_other], wog.at[:, wo_other])


    last = h_ring.arrived(half_ny)[0]
    back_own = pl.ds(pl.multiple_of(ep * cap, cap), cap)
    for sub in ORDER:
        for way in range(2):
            h_ring.serve_one(half_ny, sub, way)
        at = pl.ds(sub * sub_rows, sub_rows)
        er[at] = (oacc[at] + dot(hg[last, at], dw[weight_rows(last), :])).astype(BF16)

        def back(k, carry):
            target = lax.rem(ep + k, n_ep)
            source = pl.ds(pl.multiple_of(k * cap, cap), cap)
            for core in range(CORES):
                pltpu.make_async_remote_copy(
                    src_ref=er.at[source, pl.ds(core * mine, mine)],
                    dst_ref=ret.at[c, back_own],
                    send_sem=back_send.at[core],
                    recv_sem=back_recv.at[c],
                    device_id=(target, y * CORES + core),
                    device_id_type=MESH,
                ).start()
            return carry

        lax.fori_loop(max(1, sub * per_sub), (sub + 1) * per_sub, back, 0)
        if sub == 0:
            back_mine = pltpu.make_async_copy(
                er.at[pl.ds(0, cap), own_lanes], ret.at[c, back_own], back_local
            )
            back_mine.start()
            send_partner(9, er.at[pl.ds(0, cap), other_lanes], ret.at[c, back_own])
    back_in = to_partner(9, er.at[pl.ds(0, cap), other_lanes], ret.at[other, back_own])

    wo_in.wait_recv()
    out_part(y, True)
    for distance in range(1, 3):
        for part in a_ring.arrived(distance):
            out_part(part, False)
    for distance in range(3, half_ny):
        a_ring.serve(distance)
        for part in a_ring.arrived(distance):
            out_part(part, False)

    weight = jnp.zeros((n_ep, toks), F32)
    for k in range(topk):
        weight = weight + jnp.where(ids_ref[k : k + 1, :] == expert_idx, rw_ref[k : k + 1, :], 0.0)
    n_pieces = wide.shape[0] // CORES
    for index in range(n_pieces):
        piece = weight.astype(BF16)
        weight = weight - piece.astype(F32)
        tall = dot(spread, piece)
        for half in range(CORES):
            wide[half * n_pieces + index] = jnp.transpose(
                jnp.where(rank_tall == half * cap, tall, 0.0)
            ).astype(BF16)

    a_ring.serve(half_ny)
    out_part(a_ring.arrived(half_ny)[0], False)
    send_partner(10, ag.at[:, pl.ds(rows, shared_rows)], shp)
    shared_in = to_partner(10, ag.at[:, pl.ds(rows, shared_rows)], shp)
    out = macc[...].astype(BF16)
    mos[0] = jnp.where(c == 0, out[:, :mine], out[:, mine:])
    mos[1] = jnp.where(c == 0, out[:, mine:], out[:, :mine])
    send_partner(11, mos.at[1], mos.at[2])
    out_in = to_partner(11, mos.at[1], mos.at[2])
    mo_first = pltpu.make_async_copy(mos.at[0], mo_ref.at[own_rows], out_sem.at[0])
    mo_first.start()
    mine_sum = jnp.zeros((shared_rows, mine), F32)
    for part in range(ny):
        mine_sum = mine_sum + dot(ag[part, rows:], sdv[part * 2 * HEAD : (part + 1) * 2 * HEAD, :])
    shared_in.wait_recv()
    their_sum = jnp.zeros((shared_rows, mine), F32)
    for part in range(ny):
        their_sum = their_sum + dot(shp[part], sdv[part * 2 * HEAD : (part + 1) * 2 * HEAD, :])
    low = jnp.where(c == 0, mine_sum, their_sum)
    high = jnp.where(c == 0, their_sum, mine_sum)
    result = jnp.concatenate([low, high], axis=0)

    back_mine.wait()
    back_in.wait_recv()
    elsewhere = slots - cap
    for half in range(CORES):
        landed = ret.at[half, pl.ds(0, elsewhere)]
        pltpu.make_async_copy(landed, landed, back_recv.at[half]).wait()
    for half in range(CORES):
        for index in range(n_pieces):
            result = result + dot(wide[half * n_pieces + index], ret[half])
    eov[...] = result.astype(BF16)
    eo_out = pltpu.make_async_copy(eov, eo_ref, out_sem.at[1])
    eo_out.start()
    out_in.wait_recv()
    mo_second = pltpu.make_async_copy(mos.at[2], mo_ref.at[other_rows], out_sem.at[2])
    mo_second.start()

    for block in range(len(far_parts) + 1):
        count = elsewhere
        if block:
            count -= sub_rows * sum(not direct(block - 1, sub) for sub in range(r_subs))
        sent = og.at[block, pl.ds(0, count)]
        pltpu.make_async_copy(sent, sent, disp_send.at[block]).wait()
    for core in range(CORES):
        sent = ret.at[0, pl.ds(0, elsewhere)]
        pltpu.make_async_copy(sent, sent, back_send.at[core]).wait()
    for ring in (x_ring, r_ring, h_ring, a_ring):
        ring.finish()
    pltpu.make_async_copy(wo_z_bytes, wo_z_bytes, wo_send.at[1]).wait()
    pltpu.make_async_copy(wo_x_bytes, wo_x_bytes, wo_send.at[2]).wait()
    for copy in pending:
        copy.wait_send()

    @pl.when(jnp.logical_not(trails))
    def _():
        halo.wait_send()

    mo_first.wait()
    eo_out.wait()
    mo_second.wait()


def shards(
    mixer_input,
    mixer_gain,
    w_query,
    w_key,
    w_value,
    query_gain,
    key_gain,
    sink_logit,
    w_output,
    expert_input,
    expert_gain,
    route_ids,
    route_weight,
    expert_gate,
    expert_up,
    expert_down,
    shared_gate,
    shared_up,
    shared_down,
):
    n_ep, n_tp = lax.axis_size("ep"), lax.axis_size("tp")
    ny, nx = n_tp // CORES, min(X_SIZE, n_ep)
    rows_all, mine = mixer_input.shape
    rows = rows_all // CORES
    toks, dim = expert_input.shape
    cols = dim // ny
    slots = 2 * toks * route_ids.shape[1] // CORES
    units = expert_gate.shape[2] * CORES
    a_rows = rows + toks // CORES
    dma = pltpu.SemaphoreType.DMA
    hbm = pl.BlockSpec(memory_space=pltpu.HBM)
    anywhere = pl.BlockSpec(memory_space=pl.ANY)

    def ring_sems(subs, parts):
        return [dma(()), dma((subs * parts,))]

    return pl.pallas_call(
        functools.partial(kernel, n_ep, ny, nx),
        name="layer",
        out_shape=(
            jax.ShapeDtypeStruct((rows_all, mine), BF16),
            jax.ShapeDtypeStruct((toks, mine), BF16),
        ),
        in_specs=[hbm] * 19,
        out_specs=(anywhere, anywhere),
        scratch_shapes=[
            pltpu.VMEM((ny, rows, cols), BF16),
            pltpu.VMEM((1, dim), F32),
            pltpu.VMEM((1, HEAD), F32),
            pltpu.VMEM((1, HEAD), F32),
            pltpu.SMEM((1,), F32),
            pltpu.VMEM((1, dim), F32),
            pltpu.VMEM(route_ids.shape[::-1], jnp.int32),
            pltpu.VMEM(route_ids.shape[::-1], F32),
            pltpu.VMEM((rows, mine), BF16),
            pltpu.VMEM((toks, dim), BF16),
            pltpu.VMEM(w_key.shape, BF16),
            pltpu.VMEM(w_value.shape, BF16),
            pltpu.VMEM(w_output.shape, BF16),
            pltpu.VMEM(shared_down.shape, BF16),
            pltpu.VMEM((ny, slots, cols), BF16),
            pltpu.VMEM((ny, slots, units), BF16),
            pltpu.VMEM((ny, a_rows, 2 * HEAD), BF16),
            pltpu.VMEM((dim, units), BF16),
            pltpu.VMEM((dim, units), BF16),
            pltpu.VMEM((expert_down.shape[1], cols), BF16),
            pltpu.VMEM((2 * HEAD, dim), BF16),
            pltpu.VMEM((2 * HEAD, dim), BF16),
            pltpu.VMEM((2 * HEAD, dim), BF16),
            pltpu.VMEM((ny, 2 * w_output.shape[0], cols), BF16),
            pltpu.VMEM((ny - 2 * REACH, slots, cols), BF16),
            pltpu.VMEM((slots, cols), BF16),
            pltpu.VMEM((2, slots, mine), BF16),
            pltpu.VMEM((6, toks, slots), BF16),
            pltpu.VMEM((rows, cols), F32),
            pltpu.VMEM((toks, mine), BF16),
            pltpu.VMEM((toks, dim), BF16),
            pltpu.VMEM((slots, cols), F32),
            pltpu.VMEM((rows, 2 * HEAD), F32),
            pltpu.VMEM((rows, 2 * HEAD), F32),
            pltpu.VMEM((rows, 2 * HEAD), F32),
            pltpu.VMEM((rows, 1), F32),
            pltpu.VMEM((2, WINDOW + rows, HEAD), BF16),
            pltpu.VMEM((2, 8, 128), F32),
            pltpu.VMEM((3, rows, mine), BF16),
            pltpu.VMEM((ny, toks // CORES, 2 * HEAD), BF16),
        ]
        + ring_sems(SUBS, ny - 1)
        + ring_sems(SUBS, 2 * REACH)
        + ring_sems(SUBS, ny - 1)
        + ring_sems(2, ny - 1)
        + [
            dma((20,)),
            dma((12,)),
            dma((12,)),
            dma((ny - 2 * REACH,)),
            dma((2 * SUBS,)),
            dma((2,)),
            dma((2,)),
            dma(()),
            dma((3,)),
            dma((3,)),
            dma(()),
            dma(()),
            dma((3,)),
        ],
        compiler_params=pltpu.CompilerParams(
            collective_id=0, has_side_effects=True, vmem_limit_bytes=56 * 1024 * 1024
        ),
    )(
        mixer_input,
        mixer_gain.reshape(1, -1),
        w_query.T,
        w_key,
        w_value,
        query_gain.reshape(1, -1),
        key_gain.reshape(1, -1),
        sink_logit,
        w_output,
        expert_input,
        expert_gain.reshape(1, -1),
        route_ids.T,
        route_weight.T,
        expert_gate,
        expert_up,
        expert_down,
        shared_gate.T,
        shared_up.T,
        shared_down,
    )


def solution(mesh):
    in_specs = (
        P("ep", "tp"),
        P(),
        P(None, "tp"),
        P(),
        P(),
        P(),
        P(),
        P("tp"),
        P("tp", None),
        P("ep", None),
        P(),
        P("ep", None),
        P("ep", None),
        P("ep", None, "tp"),
        P("ep", None, "tp"),
        P("ep", None, "tp"),
        P(None, "tp"),
        P(None, "tp"),
        P(None, "tp"),
    )
    out_specs = (P("ep", "tp"), P("ep", "tp"))
    return jax.shard_map(shards, mesh=mesh, in_specs=in_specs, out_specs=out_specs, check_vma=False)
```

```python
import functools

import jax
import jax.numpy as jnp
from jax import lax
from jax.experimental import pallas as pl
from jax.experimental.pallas import tpu as pltpu
from jax.sharding import PartitionSpec as P

HEAD = 64
WINDOW = 128
EPSILON = 1e-06
CORES = 2
X_SIZE = 4
REACH = 2
SUBS = 4
ORDER = (0, 3, 1, 2)
FURTHER = ()
PAIR_SEM = {1: 0, 2: 0, 7: 0, 3: 1, 4: 1, 5: 1, 8: 1, 0: 2, 10: 2, 11: 2, 6: 3, 9: 3}
F32 = jnp.float32
BF16 = jnp.bfloat16
MESH = pl.DeviceIdType.MESH


def mod(value, count):
    return lax.rem(value + count, count)


def dot(a, b):
    return jnp.dot(a, b, preferred_element_type=F32)


def dot_rows(a, b):
    return lax.dot_general(a, b, (((1,), (1,)), ((), ())), preferred_element_type=F32)


class Ring:
    def __init__(self, buf, send_sem, recv_sem, y, ny, place, subs, reach=None, further=()):
        self.further = further
        self.buf, self.send_sem, self.recv_sem = buf, send_sem, recv_sem
        self.y, self.ny, self.place = y, ny, place
        self.subs, self.reach = subs, reach
        self.half = ny // 2
        self.rows = buf.shape[1] // subs

    def carries(self, way, distance, sub):
        if self.reach is not None:
            return distance <= self.reach + (sub in self.further)
        if distance < self.half:
            return True
        if distance > self.half:
            return False
        return (sub < self.subs // 2) == (way == 0)

    def copy(self, way, distance, sub, origin):
        sign = 1 if way == 0 else -1
        part = mod(self.y - sign * origin, self.ny)
        rows = pl.ds(sub * self.rows, self.rows)
        index = (distance - 1) * self.subs * 2 + sub * 2 + way
        if self.reach is None and distance == self.half:
            index = (distance - 1) * self.subs * 2 + sub
        return pltpu.make_async_remote_copy(
            src_ref=self.buf.at[part, rows],
            dst_ref=self.buf.at[part, rows],
            send_sem=self.send_sem,
            recv_sem=self.recv_sem.at[index],
            device_id=self.place(mod(self.y + sign, self.ny)),
            device_id_type=MESH,
        )

    def send(self, distance, sub, way):
        if self.carries(way, distance, sub):
            self.copy(way, distance, sub, distance - 1).start()

    def start(self, sub):
        for way in range(2):
            self.send(1, sub, way)

    def serve_one(self, distance, sub, way):
        if self.carries(way, distance, sub):
            self.copy(way, distance, sub, distance).wait_recv()
            self.send(distance + 1, sub, way)

    def serve(self, distance, order=None):
        for sub in order or range(self.subs):
            for way in range(2):
                self.serve_one(distance, sub, way)

    def arrived(self, distance):
        if distance < self.half:
            return [mod(self.y - distance, self.ny), mod(self.y + distance, self.ny)]
        return [mod(self.y - distance, self.ny)]

    def finish(self):
        pieces = (self.ny - 1) * self.subs
        if self.reach is not None:
            pieces = 2 * (self.reach * self.subs + len(self.further))
        high = max(k for k in range(1, self.subs + 1) if pieces % k == 0)
        sent = self.buf.at[pl.ds(0, pieces // high), pl.ds(0, high * self.rows)]
        pltpu.make_async_copy(sent, sent, self.send_sem).wait()


def kernel(
    n_ep,
    ny,
    nx,
    x_ref,
    gain_in,
    wq_ref,
    wk_ref,
    wv_ref,
    qg_in,
    kg_in,
    sink_in,
    wo_ref,
    ei_ref,
    eg_in,
    ids_in,
    rw_in,
    gate_ref,
    up_ref,
    down_ref,
    sg_ref,
    su_ref,
    sd_ref,
    mo_ref,
    eo_ref,
    xg,
    gain_ref,
    qg_ref,
    kg_ref,
    sink_ref,
    eg_ref,
    ids_ref,
    rw_ref,
    xv,
    eiv,
    wkv,
    wvv,
    wov,
    sdv,
    rg,
    hg,
    ag,
    gw,
    uw,
    dw,
    wqs,
    sgs,
    sus,
    wog,
    og,
    er,
    ret,
    wide,
    macc,
    eov,
    normed,
    oacc,
    qacc,
    kacc,
    vacc,
    ssq,
    kv,
    sk,
    mos,
    shp,
    xs_sem,
    xr_sem,
    rs_sem,
    rr_sem,
    hs_sem,
    hr_sem,
    as_sem,
    ar_sem,
    local_sem,
    pair_send,
    pair_recv,
    disp_send,
    disp_recv,
    back_send,
    back_recv,
    back_local,
    wo_send,
    wo_recv,
    halo_send,
    halo_recv,
    out_sem,
):
    ep = lax.axis_index("ep")
    tp = lax.axis_index("tp")
    y = tp // CORES
    c = lax.rem(tp, CORES)
    other = 1 - c
    half_ny = ny // 2
    rows = x_ref.shape[0] // CORES
    toks = ei_ref.shape[0]
    dim = ei_ref.shape[1]
    cols = dim // ny
    mine = dim // (ny * CORES)
    cap = er.shape[0] // n_ep
    slots = er.shape[0]
    xi = lax.rem(ep, nx)
    far_parts = [mod(y + REACH + 1 + k, ny) for k in range(ny - 1 - 2 * REACH)]

    def here(place):
        return (ep, place * CORES + c)

    partner = (ep, y * CORES + other)

    own_lanes = pl.ds(pl.multiple_of(c * mine, mine), mine)
    other_lanes = pl.ds(pl.multiple_of(other * mine, mine), mine)
    own_head = pl.ds(pl.multiple_of(c * HEAD, HEAD), HEAD)
    other_head = pl.ds(pl.multiple_of(other * HEAD, HEAD), HEAD)
    own_rows = pl.ds(pl.multiple_of(c * rows, rows), rows)
    other_rows = pl.ds(pl.multiple_of(other * rows, rows), rows)
    wo_rows = wo_ref.shape[0]
    wo_piece = wo_rows // nx
    wo_src = pl.ds(pl.multiple_of(xi * wo_piece, wo_piece), wo_piece)
    wo_dst = pl.ds(pl.multiple_of(c * wo_rows + xi * wo_piece, wo_piece), wo_piece)
    wo_own = pl.ds(pl.multiple_of(c * wo_rows, wo_rows), wo_rows)
    wo_other = pl.ds(pl.multiple_of(other * wo_rows, wo_rows), wo_rows)

    def lanes_of(part):
        return pl.ds(pl.multiple_of(part * cols, cols), cols)

    def load(index, source, target):
        copy = pltpu.make_async_copy(source, target, local_sem.at[index])
        copy.start()
        return copy

    ids_load = load(13, ids_in, ids_ref)
    ei_in = load(0, ei_ref, eiv)
    eg_load = load(14, eg_in, eg_ref)
    xv_in = load(1, x_ref.at[other_rows], xv)
    x_own_in = load(2, x_ref.at[own_rows], xg.at[y, :, own_lanes])
    wov_in = load(3, wo_ref, wov)
    sink_load = load(19, sink_in, sink_ref)

    barrier = pltpu.get_barrier_semaphore()

    def greet(k, carry):
        target = lax.rem(ep + k, n_ep)
        for core in range(CORES):
            pl.semaphore_signal(
                barrier, inc=1, device_id=(target, y * CORES + core), device_id_type=MESH
            )
        return carry

    lax.fori_loop(n_ep // 4, n_ep, greet, 0)
    lax.fori_loop(1, n_ep // 4, greet, 0)
    for k in range(1, ny):
        pl.semaphore_signal(barrier, inc=1, device_id=here(mod(y + k, ny)), device_id_type=MESH)
    pl.semaphore_signal(barrier, inc=1, device_id=partner, device_id_type=MESH)
    small = [
        load(15, rw_in, rw_ref),
        load(16, gain_in, gain_ref),
        load(17, qg_in, qg_ref),
        load(18, kg_in, kg_ref),
    ]
    weights_in = [
        load(4, wq_ref, wqs.at[own_head]),
        load(5, wk_ref, wkv),
        load(6, wv_ref, wvv),
        load(7, gate_ref.at[0], gw.at[:, own_lanes]),
        load(8, up_ref.at[0], uw.at[:, own_lanes]),
        load(9, sg_ref, sgs.at[own_head]),
        load(10, su_ref, sus.at[own_head]),
        load(11, down_ref.at[0], dw.at[:, own_lanes]),
        load(12, sd_ref, sdv),
    ]
    sink_load.wait()
    sk[c] = jnp.full((8, 128), sink_ref[0], F32)

    ids_load.wait()
    topk = ids_ref.shape[0]
    expert_idx = lax.broadcasted_iota(jnp.int32, (n_ep, toks), 0)
    named = jnp.zeros((n_ep, toks), F32)
    for k in range(topk):
        named = named + jnp.where(ids_ref[k : k + 1, :] == expert_idx, 1.0, 0.0)
    t_row = lax.broadcasted_iota(jnp.int32, (toks, toks), 0)
    t_col = lax.broadcasted_iota(jnp.int32, (toks, toks), 1)
    before = jnp.where(t_row < t_col, 1.0, 0.0).astype(BF16)
    rank = dot(named.astype(BF16), before)
    rank = jnp.where(named > 0.0, rank, -1.0)
    e_row = lax.broadcasted_iota(jnp.int32, (slots, n_ep), 0)
    e_col = lax.broadcasted_iota(jnp.int32, (slots, n_ep), 1)
    spread = jnp.where(e_row // cap == e_col, 1.0, 0.0).astype(BF16)
    slot_row = lax.rem(lax.broadcasted_iota(jnp.int32, (slots, toks), 0), cap)
    rank_tall = dot(spread, rank.astype(BF16)).astype(jnp.int32) - slot_row
    pick = jnp.where(rank_tall == c * cap, 1.0, 0.0).astype(BF16)
    ei_in.wait()
    eg_load.wait()
    expert_float = eiv[...].astype(F32)
    squares = jnp.mean(expert_float * expert_float, axis=-1, keepdims=True)
    normed[...] = (expert_float * lax.rsqrt(squares + EPSILON) * eg_ref[...]).astype(BF16)
    og[0] = dot(pick, normed[:, lanes_of(y)]).astype(BF16)
    xv_in.wait()
    x_own_in.wait()

    pl.semaphore_wait(barrier, (n_ep - 1) * CORES + (ny - 1) + 1)

    def to_partner(index, source, target):
        return pltpu.make_async_remote_copy(
            src_ref=source,
            dst_ref=target,
            send_sem=pair_send.at[PAIR_SEM[index]],
            recv_sem=pair_recv.at[index],
            device_id=partner,
            device_id_type=MESH,
        )

    def send_partner(index, source, target):
        to_partner(index, source, target).start()

    send_partner(0, xv, xg.at[y, :, own_lanes])
    x_in = to_partner(0, xv, xg.at[y, :, other_lanes])

    zi = ep // nx
    nz = n_ep // nx
    away = zi > 0
    wov_in.wait()
    wo_place = mod(y + zi, ny)
    wo_self = pltpu.make_async_copy(
        wov.at[wo_src, lanes_of(wo_place)], wog.at[y, wo_dst], local_sem.at[3]
    )
    wo_y = pltpu.make_async_remote_copy(
        src_ref=wov.at[wo_src, lanes_of(wo_place)],
        dst_ref=wog.at[y, wo_dst],
        send_sem=wo_send.at[0],
        recv_sem=wo_recv.at[0],
        device_id=here(wo_place),
        device_id_type=MESH,
    )

    @pl.when(away)
    def _():
        wo_y.start()

    @pl.when(jnp.logical_not(away))
    def _():
        wo_self.start()

    r_subs = SUBS
    sub_rows = slots // r_subs
    per_sub = n_ep // r_subs

    def direct(far, sub):
        return sub not in FURTHER or 0 < far < len(far_parts) - 1

    def dispatch(blocks, parts, base):
        for block, part in zip(blocks, parts):
            pltpu.make_async_copy(
                og.at[block, pl.ds(pl.multiple_of(ep * cap, cap), cap)],
                rg.at[part, pl.ds(0, cap)],
                disp_recv.at[base],
            ).start()

        for sub in ORDER:

            def send(k, carry, sub=sub):
                target = lax.rem(ep + n_ep - k, n_ep)
                for block, part in zip(blocks, parts):
                    if base and not direct(block - 1, sub):
                        continue
                    pltpu.make_async_remote_copy(
                        src_ref=og.at[block, pl.ds(pl.multiple_of(target * cap, cap), cap)],
                        dst_ref=rg.at[part, pl.ds(pl.multiple_of(k * cap, cap), cap)],
                        send_sem=disp_send.at[block],
                        recv_sem=disp_recv.at[base + sub],
                        device_id=(target, tp),
                        device_id_type=MESH,
                    ).start()
                return carry

            lax.fori_loop(max(1, sub * per_sub), (sub + 1) * per_sub, send, 0)

    dispatch([0], [y], 0)

    x_ring = Ring(xg, xs_sem, xr_sem, y, ny, here, 4)
    x_in.wait_recv()
    for sub in range(x_ring.subs):
        x_ring.start(sub)

    for k, part in enumerate(far_parts):
        og[k + 1] = dot(pick, normed[:, lanes_of(part)]).astype(BF16)
    dispatch(range(1, len(far_parts) + 1), far_parts, r_subs)

    for copy in weights_in + small:
        copy.wait()
    send_partner(3, wqs.at[own_head], wqs.at[own_head])
    send_partner(6, sk.at[c], sk.at[c])
    wq_in = to_partner(3, wqs.at[own_head], wqs.at[other_head])
    sk_in = to_partner(6, sk.at[c], sk.at[other])

    x_ring.serve(1)

    send_partner(1, gw.at[:, own_lanes], gw.at[:, own_lanes])
    send_partner(2, uw.at[:, own_lanes], uw.at[:, own_lanes])
    gw_in = to_partner(1, gw.at[:, own_lanes], gw.at[:, other_lanes])
    uw_in = to_partner(2, uw.at[:, own_lanes], uw.at[:, other_lanes])

    r_ring = Ring(rg, rs_sem, rr_sem, y, ny, here, r_subs, REACH, FURTHER)

    def r_start(sub):
        landed = rg.at[y, pl.ds(sub * per_sub * cap, per_sub * cap)]
        pltpu.make_async_copy(landed, landed, disp_recv.at[sub]).wait()
        r_ring.start(sub)

    r_start(ORDER[0])

    x_ring.serve(2)

    for sub in ORDER[1:]:
        r_start(sub)

    x_ring.serve(3)
    send_partner(4, sgs.at[own_head], sgs.at[own_head])
    send_partner(5, sus.at[own_head], sus.at[own_head])
    send_partner(7, dw.at[:, own_lanes], dw.at[:, own_lanes])
    sg_in = to_partner(4, sgs.at[own_head], sgs.at[other_head])
    su_in = to_partner(5, sus.at[own_head], sus.at[other_head])
    dw_in = to_partner(7, dw.at[:, own_lanes], dw.at[:, other_lanes])

    for distance in range(1, REACH):
        r_ring.serve(distance, ORDER)
    def weight_rows(part):
        return pl.ds(pl.multiple_of(part * cols, cols), cols)

    h_ring = Ring(hg, hs_sem, hr_sem, y, ny, here, r_subs)
    near_parts = [y]
    for distance in range(1, REACH + 1):
        near_parts += r_ring.arrived(distance)

    def hidden(sub):
        for way in range(2):
            if sub in FURTHER:
                r_ring.serve_one(REACH + 1, sub, way)
            else:
                r_ring.serve_one(REACH, sub, way)
        n_direct = sum(direct(far, sub) for far in range(len(far_parts)))
        landed = rg.at[pl.ds(0, n_direct), pl.ds(0, sub_rows)]
        pltpu.make_async_copy(landed, landed, disp_recv.at[r_subs + sub]).wait()
        at = pl.ds(sub * sub_rows, sub_rows)
        gate_pre = jnp.zeros((sub_rows, gw.shape[1]), F32)
        up_pre = jnp.zeros((sub_rows, uw.shape[1]), F32)
        for part in near_parts + far_parts:
            portion = rg[part, at]
            gate_pre = gate_pre + dot(portion, gw[weight_rows(part), :])
            up_pre = up_pre + dot(portion, uw[weight_rows(part), :])
        hg[y, at] = (jax.nn.silu(gate_pre) * up_pre).astype(BF16)
        h_ring.start(sub)

    gw_in.wait_recv()
    uw_in.wait_recv()
    hidden(ORDER[0])

    for distance in range(4, half_ny + 1):
        x_ring.serve(distance)

    wq_in.wait_recv()
    qacc[...] = jnp.zeros_like(qacc)
    kacc[...] = jnp.zeros_like(kacc)
    vacc[...] = jnp.zeros_like(vacc)
    ssq[...] = jnp.zeros_like(ssq)

    def project(part, carry):
        lanes = lanes_of(part)
        portion = xg[part].astype(F32)
        scaled = (portion * gain_ref[:, lanes]).astype(BF16)
        ssq[...] += jnp.sum(portion * portion, axis=-1, keepdims=True)
        qacc[...] += dot_rows(scaled, wqs[:, lanes])
        kacc[...] += dot(scaled, wkv[lanes, :])
        vacc[...] += dot(scaled, wvv[lanes, :])
        return carry

    lax.fori_loop(0, ny // 2, project, 0)

    hidden(ORDER[1])

    lax.fori_loop(ny // 2, ny, project, 0)
    first_kv = y < ny // 2

    def head_of(both):
        return jnp.where(first_kv, both[:, :HEAD], both[:, HEAD:])

    def head_norm(raw, gain):
        return raw * lax.rsqrt(jnp.mean(raw * raw, axis=-1, keepdims=True) + EPSILON) * gain

    inv_rms = lax.rsqrt(ssq[...] / dim + EPSILON)
    keys = head_norm(head_of(kacc[...]), kg_ref[...]).astype(BF16)
    values = (head_of(vacc[...]) * inv_rms).astype(BF16)
    kv[0, WINDOW:] = keys
    kv[1, WINDOW:] = values

    leads = jnp.logical_and(ep == 0, c == 0)
    trails = jnp.logical_and(ep == n_ep - 1, c == CORES - 1)
    after_ep = jnp.where(c == CORES - 1, lax.rem(ep + 1, n_ep), ep)
    halo = pltpu.make_async_remote_copy(
        src_ref=kv.at[:, pl.ds(rows, WINDOW)],
        dst_ref=kv.at[:, pl.ds(0, WINDOW)],
        send_sem=halo_send,
        recv_sem=halo_recv,
        device_id=(after_ep, y * CORES + other),
        device_id_type=MESH,
    )

    @pl.when(jnp.logical_not(trails))
    def _():
        halo.start()

    @pl.when(leads)
    def _():
        kv[:, :WINDOW] = jnp.zeros((2, WINDOW, HEAD), BF16)

    for sub in FURTHER:
        for way in range(2):
            r_ring.serve_one(REACH, sub, way)

    hidden(ORDER[2])
    h_ring.serve(1, ORDER[:2])

    sg_in.wait_recv()
    su_in.wait_recv()
    shared_rows = toks // CORES
    own_toks = normed[pl.ds(pl.multiple_of(c * shared_rows, shared_rows), shared_rows)]
    gate_pre = dot_rows(own_toks, sgs[...])
    up_pre = dot_rows(own_toks, sus[...])
    ag[y, rows:] = (jax.nn.silu(gate_pre) * up_pre).astype(BF16)

    q_idx = lax.broadcasted_iota(jnp.int32, (WINDOW, 2 * WINDOW), 0)
    k_idx = lax.broadcasted_iota(jnp.int32, (WINDOW, 2 * WINDOW), 1)
    relative = q_idx + WINDOW - k_idx
    near = jnp.logical_and(relative >= 0, relative < WINDOW)
    first_key = jnp.where(leads, WINDOW, 0)

    @pl.when(jnp.logical_not(leads))
    def _():
        halo.wait_recv()

    sk_in.wait_recv()

    def attend(block):
        start = block * WINDOW
        allowed = near
        if block == 0:
            allowed = jnp.logical_and(near, k_idx >= first_key)
        heads = []
        for head in range(2):
            raw = qacc[start : start + WINDOW, head * HEAD : (head + 1) * HEAD]
            queries = head_norm(raw, qg_ref[...]).astype(BF16)
            sink = sk[head, 0:1, 0:1]
            scores = dot_rows(queries, kv[0, start : start + 2 * WINDOW]) * HEAD ** (-0.5)
            masked = jnp.where(allowed, scores, -jnp.inf)
            peak = jnp.maximum(jnp.max(masked, axis=-1, keepdims=True), sink)
            exponent = jnp.exp(masked - peak)
            denominator = jnp.sum(exponent, axis=-1, keepdims=True) + jnp.exp(sink - peak)
            probs = (exponent / denominator).astype(BF16)
            heads.append(dot(probs, kv[1, start : start + 2 * WINDOW]))
        ag[y, start : start + WINDOW] = jnp.concatenate(heads, axis=1).astype(BF16)

    wo_part = mod(y - zi, ny)

    @pl.when(away)
    def _():
        wo_y.wait()

    @pl.when(jnp.logical_not(away))
    def _():
        wo_self.wait()

    wo_z_bytes = og.at[0, pl.ds(0, (nz - 1) * wo_piece)]
    for k in range(1, nz):
        pltpu.make_async_remote_copy(
            src_ref=wog.at[wo_part, wo_dst],
            dst_ref=wog.at[wo_part, wo_dst],
            send_sem=wo_send.at[1],
            recv_sem=wo_recv.at[1],
            device_id=(lax.rem(ep + k * nx, n_ep), tp),
            device_id_type=MESH,
        ).start()

    for block in range(rows // WINDOW):
        attend(block)

    a_ring = Ring(ag, as_sem, ar_sem, y, ny, here, 2)
    for sub in range(a_ring.subs):
        a_ring.start(sub)

    hidden(ORDER[3])

    h_ring.serve(1, ORDER[2:3])
    h_ring.serve(2, ORDER[:2])
    h_ring.serve(1, ORDER[3:])
    h_ring.serve(2, ORDER[2:])

    pltpu.make_async_copy(wo_z_bytes, wo_z_bytes, wo_recv.at[1]).wait()
    wo_x_bytes = wog.at[:, pl.ds(0, (nx - 1) * wo_piece)]
    for k in range(1, nx):
        pltpu.make_async_remote_copy(
            src_ref=wog.at[:, wo_dst],
            dst_ref=wog.at[:, wo_dst],
            send_sem=wo_send.at[2],
            recv_sem=wo_recv.at[2],
            device_id=(ep - xi + lax.rem(xi + k, nx), tp),
            device_id_type=MESH,
        ).start()

    def out_part(part, first):
        total = dot(ag[part, :rows], wog[part])
        if first:
            macc[...] = total
        else:
            macc[...] += total

    a_ring.serve(1)
    dw_in.wait_recv()

    seven = [y]
    for distance in range(1, half_ny):
        seven += h_ring.arrived(distance)
    for distance in range(3, half_ny):
        for sub in ORDER:
            h_ring.serve(distance, (sub,))
            at = pl.ds(sub * sub_rows, sub_rows)
            total = jnp.zeros((sub_rows, cols), F32)
            for part in seven:
                total = total + dot(hg[part, at], dw[weight_rows(part), :])
            oacc[at] = total
    a_ring.serve(2)

    pltpu.make_async_copy(wo_x_bytes, wo_x_bytes, wo_recv.at[2]).wait()
    send_partner(8, wog.at[:, wo_own], wog.at[:, wo_own])
    wo_in = to_partner(8, wog.at[:, wo_other], wog.at[:, wo_other])


    last = h_ring.arrived(half_ny)[0]
    back_own = pl.ds(pl.multiple_of(ep * cap, cap), cap)
    for sub in ORDER:
        for way in range(2):
            h_ring.serve_one(half_ny, sub, way)
        at = pl.ds(sub * sub_rows, sub_rows)
        er[at] = (oacc[at] + dot(hg[last, at], dw[weight_rows(last), :])).astype(BF16)

        def back(k, carry):
            target = lax.rem(ep + k, n_ep)
            source = pl.ds(pl.multiple_of(k * cap, cap), cap)
            for core in range(CORES):
                pltpu.make_async_remote_copy(
                    src_ref=er.at[source, pl.ds(core * mine, mine)],
                    dst_ref=ret.at[c, back_own],
                    send_sem=back_send.at[core],
                    recv_sem=back_recv.at[c],
                    device_id=(target, y * CORES + core),
                    device_id_type=MESH,
                ).start()
            return carry

        lax.fori_loop(max(1, sub * per_sub), (sub + 1) * per_sub, back, 0)
        if sub == 0:
            back_mine = pltpu.make_async_copy(
                er.at[pl.ds(0, cap), own_lanes], ret.at[c, back_own], back_local
            )
            back_mine.start()
            send_partner(9, er.at[pl.ds(0, cap), other_lanes], ret.at[c, back_own])
    back_in = to_partner(9, er.at[pl.ds(0, cap), other_lanes], ret.at[other, back_own])

    wo_in.wait_recv()
    out_part(y, True)
    for distance in range(1, 3):
        for part in a_ring.arrived(distance):
            out_part(part, False)
    for distance in range(3, half_ny):
        a_ring.serve(distance)
        for part in a_ring.arrived(distance):
            out_part(part, False)

    weight = jnp.zeros((n_ep, toks), F32)
    for k in range(topk):
        weight = weight + jnp.where(ids_ref[k : k + 1, :] == expert_idx, rw_ref[k : k + 1, :], 0.0)
    n_pieces = wide.shape[0] // CORES
    for index in range(n_pieces):
        piece = weight.astype(BF16)
        weight = weight - piece.astype(F32)
        tall = dot(spread, piece)
        for half in range(CORES):
            wide[half * n_pieces + index] = jnp.transpose(
                jnp.where(rank_tall == half * cap, tall, 0.0)
            ).astype(BF16)

    a_ring.serve(half_ny)
    out_part(a_ring.arrived(half_ny)[0], False)
    send_partner(10, ag.at[:, pl.ds(rows, shared_rows)], shp)
    shared_in = to_partner(10, ag.at[:, pl.ds(rows, shared_rows)], shp)
    out = macc[...].astype(BF16)
    mos[0] = jnp.where(c == 0, out[:, :mine], out[:, mine:])
    mos[1] = jnp.where(c == 0, out[:, mine:], out[:, :mine])
    send_partner(11, mos.at[1], mos.at[2])
    out_in = to_partner(11, mos.at[1], mos.at[2])
    mo_first = pltpu.make_async_copy(mos.at[0], mo_ref.at[own_rows], out_sem.at[0])
    mo_first.start()
    mine_sum = jnp.zeros((shared_rows, mine), F32)
    for part in range(ny):
        mine_sum = mine_sum + dot(ag[part, rows:], sdv[part * 2 * HEAD : (part + 1) * 2 * HEAD, :])
    shared_in.wait_recv()
    their_sum = jnp.zeros((shared_rows, mine), F32)
    for part in range(ny):
        their_sum = their_sum + dot(shp[part], sdv[part * 2 * HEAD : (part + 1) * 2 * HEAD, :])
    low = jnp.where(c == 0, mine_sum, their_sum)
    high = jnp.where(c == 0, their_sum, mine_sum)
    result = jnp.concatenate([low, high], axis=0)

    back_mine.wait()
    back_in.wait_recv()
    elsewhere = slots - cap
    for half in range(CORES):
        landed = ret.at[half, pl.ds(0, elsewhere)]
        pltpu.make_async_copy(landed, landed, back_recv.at[half]).wait()
    for half in range(CORES):
        for index in range(n_pieces):
            result = result + dot(wide[half * n_pieces + index], ret[half])
    eov[...] = result.astype(BF16)
    eo_out = pltpu.make_async_copy(eov, eo_ref, out_sem.at[1])
    eo_out.start()
    out_in.wait_recv()
    mo_second = pltpu.make_async_copy(mos.at[2], mo_ref.at[other_rows], out_sem.at[2])
    mo_second.start()

    for block in range(len(far_parts) + 1):
        count = elsewhere
        if block:
            count -= sub_rows * sum(not direct(block - 1, sub) for sub in range(r_subs))
        sent = og.at[block, pl.ds(0, count)]
        pltpu.make_async_copy(sent, sent, disp_send.at[block]).wait()
    for core in range(CORES):
        sent = ret.at[0, pl.ds(0, elsewhere)]
        pltpu.make_async_copy(sent, sent, back_send.at[core]).wait()
    for ring in (x_ring, r_ring, h_ring, a_ring):
        ring.finish()
    pltpu.make_async_copy(wo_z_bytes, wo_z_bytes, wo_send.at[1]).wait()
    pltpu.make_async_copy(wo_x_bytes, wo_x_bytes, wo_send.at[2]).wait()
    pair_sent = [hg.at[pl.ds(0, 6)], hg.at[pl.ds(0, 4)], hg.at[0], og.at[0, pl.ds(0, 16)]]
    for index, sent in enumerate(pair_sent):
        pltpu.make_async_copy(sent, sent, pair_send.at[index]).wait()

    @pl.when(jnp.logical_not(trails))
    def _():
        halo.wait_send()

    mo_first.wait()
    eo_out.wait()
    mo_second.wait()


def shards(
    mixer_input,
    mixer_gain,
    w_query,
    w_key,
    w_value,
    query_gain,
    key_gain,
    sink_logit,
    w_output,
    expert_input,
    expert_gain,
    route_ids,
    route_weight,
    expert_gate,
    expert_up,
    expert_down,
    shared_gate,
    shared_up,
    shared_down,
):
    n_ep, n_tp = lax.axis_size("ep"), lax.axis_size("tp")
    ny, nx = n_tp // CORES, min(X_SIZE, n_ep)
    rows_all, mine = mixer_input.shape
    rows = rows_all // CORES
    toks, dim = expert_input.shape
    cols = dim // ny
    slots = 2 * toks * route_ids.shape[1] // CORES
    units = expert_gate.shape[2] * CORES
    a_rows = rows + toks // CORES
    dma = pltpu.SemaphoreType.DMA
    hbm = pl.BlockSpec(memory_space=pltpu.HBM)
    anywhere = pl.BlockSpec(memory_space=pl.ANY)

    def ring_sems(subs, parts):
        return [dma(()), dma((subs * parts,))]

    return pl.pallas_call(
        functools.partial(kernel, n_ep, ny, nx),
        name="layer",
        out_shape=(
            jax.ShapeDtypeStruct((rows_all, mine), BF16),
            jax.ShapeDtypeStruct((toks, mine), BF16),
        ),
        in_specs=[hbm] * 19,
        out_specs=(anywhere, anywhere),
        scratch_shapes=[
            pltpu.VMEM((ny, rows, cols), BF16),
            pltpu.VMEM((1, dim), F32),
            pltpu.VMEM((1, HEAD), F32),
            pltpu.VMEM((1, HEAD), F32),
            pltpu.SMEM((1,), F32),
            pltpu.VMEM((1, dim), F32),
            pltpu.VMEM(route_ids.shape[::-1], jnp.int32),
            pltpu.VMEM(route_ids.shape[::-1], F32),
            pltpu.VMEM((rows, mine), BF16),
            pltpu.VMEM((toks, dim), BF16),
            pltpu.VMEM(w_key.shape, BF16),
            pltpu.VMEM(w_value.shape, BF16),
            pltpu.VMEM(w_output.shape, BF16),
            pltpu.VMEM(shared_down.shape, BF16),
            pltpu.VMEM((ny, slots, cols), BF16),
            pltpu.VMEM((ny, slots, units), BF16),
            pltpu.VMEM((ny, a_rows, 2 * HEAD), BF16),
            pltpu.VMEM((dim, units), BF16),
            pltpu.VMEM((dim, units), BF16),
            pltpu.VMEM((expert_down.shape[1], cols), BF16),
            pltpu.VMEM((2 * HEAD, dim), BF16),
            pltpu.VMEM((2 * HEAD, dim), BF16),
            pltpu.VMEM((2 * HEAD, dim), BF16),
            pltpu.VMEM((ny, 2 * w_output.shape[0], cols), BF16),
            pltpu.VMEM((ny - 2 * REACH, slots, cols), BF16),
            pltpu.VMEM((slots, cols), BF16),
            pltpu.VMEM((2, slots, mine), BF16),
            pltpu.VMEM((6, toks, slots), BF16),
            pltpu.VMEM((rows, cols), F32),
            pltpu.VMEM((toks, mine), BF16),
            pltpu.VMEM((toks, dim), BF16),
            pltpu.VMEM((slots, cols), F32),
            pltpu.VMEM((rows, 2 * HEAD), F32),
            pltpu.VMEM((rows, 2 * HEAD), F32),
            pltpu.VMEM((rows, 2 * HEAD), F32),
            pltpu.VMEM((rows, 1), F32),
            pltpu.VMEM((2, WINDOW + rows, HEAD), BF16),
            pltpu.VMEM((2, 8, 128), F32),
            pltpu.VMEM((3, rows, mine), BF16),
            pltpu.VMEM((ny, toks // CORES, 2 * HEAD), BF16),
        ]
        + ring_sems(SUBS, ny - 1)
        + ring_sems(SUBS, 2 * REACH)
        + ring_sems(SUBS, ny - 1)
        + ring_sems(2, ny - 1)
        + [
            dma((20,)),
            dma((4,)),
            dma((12,)),
            dma((ny - 2 * REACH,)),
            dma((2 * SUBS,)),
            dma((2,)),
            dma((2,)),
            dma(()),
            dma((3,)),
            dma((3,)),
            dma(()),
            dma(()),
            dma((3,)),
        ],
        compiler_params=pltpu.CompilerParams(
            collective_id=0, has_side_effects=True, vmem_limit_bytes=56 * 1024 * 1024
        ),
    )(
        mixer_input,
        mixer_gain.reshape(1, -1),
        w_query.T,
        w_key,
        w_value,
        query_gain.reshape(1, -1),
        key_gain.reshape(1, -1),
        sink_logit,
        w_output,
        expert_input,
        expert_gain.reshape(1, -1),
        route_ids.T,
        route_weight.T,
        expert_gate,
        expert_up,
        expert_down,
        shared_gate.T,
        shared_up.T,
        shared_down,
    )


def solution(mesh):
    in_specs = (
        P("ep", "tp"),
        P(),
        P(None, "tp"),
        P(),
        P(),
        P(),
        P(),
        P("tp"),
        P("tp", None),
        P("ep", None),
        P(),
        P("ep", None),
        P("ep", None),
        P("ep", None, "tp"),
        P("ep", None, "tp"),
        P("ep", None, "tp"),
        P(None, "tp"),
        P(None, "tp"),
        P(None, "tp"),
    )
    out_specs = (P("ep", "tp"), P("ep", "tp"))
    return jax.shard_map(shards, mesh=mesh, in_specs=in_specs, out_specs=out_specs, check_vma=False)
```
